32 devices in a mesh: sp: 4 (over z), fs: 4 (over y, x), tp: 2 (over core).
Axes of the slice: x: 2, y: 2, z: 4, core: 2. Of those that a mesh axis runs over, the one named last changes fastest.
Arguments:
- tokens: bfloat16 [4, 1024, 2048], P('fs', ('sp', 'tp')), may hold values from -6 to 6
- h_gain: float32 [2048], replicated, may hold values from 0.1 to 1.9
- w_qlat: bfloat16 [2048, 768], P(('sp', 'fs')), may hold values from -0.125 to 0.125
- w_kvlat: bfloat16 [2048, 512], P(('sp', 'fs')), may hold values from -0.125 to 0.125
- w_krope: bfloat16 [2048, 32], P(('sp', 'fs')), may hold values from -0.125 to 0.125
- q_gain: float32 [768], replicated, may hold values from 0.3 to 4.5, as said below
- kv_gain: float32 [512], replicated, may hold values from 0.3 to 4.5, as said below
- w_uq: bfloat16 [768, 1536], P(None, 'tp'), may hold values from -0.375 to 0.375
- w_uk: bfloat16 [512, 1024], P(None, 'tp'), may hold values from -0.4375 to 0.4375
- w_uv: bfloat16 [512, 1024], P(None, 'tp'), may hold values from -0.25 to 0.25
- w_convb: bfloat16 [2048, 1024], P(None, 'tp'), may hold values from -0.125 to 0.125
- w_convc: bfloat16 [2048, 1024], P(None, 'tp'), may hold values from -0.125 to 0.125
- w_convx: bfloat16 [2048, 1024], P(None, 'tp'), may hold values from -0.125 to 0.125
- conv_taps: float32 [3, 1024], P(None, 'tp'), may hold values from -3 to 3
- w_out_attn: bfloat16 [1024, 2048], P('tp'), may hold values from -0.125 to 0.125
- w_out_conv: bfloat16 [1024, 2048], P('tp'), may hold values from -0.125 to 0.125
Outputs:
- mixed: bfloat16 [4, 1024, 2048], P('fs', ('sp', 'tp'))
The draws below stay inside these ranges and needn't reach their ends.
Inputs may be any that keep to these rules, and one draw needn't show every extreme that they name: `q_gain`: positive gains of the query latent's norm. `kv_gain`: positive gains of the key-value latent's norm.
All inputs are finite; a program needn't handle non-finite values.
Results may differ from the reference program's by a relative error of at most 0.017.
The reference program's roundings to bfloat16 on the way count: a program that leaves them out, or rounds other values in their place, can miss the bound.
Values may be sent and summed in bfloat16 or wider, within the bound.
A program may use at most 64 MiB of HBM per device.

```python
import jax
import jax.numpy as jnp
from jax import lax

D = 2048
H = 16
QR = 768
KVR = 512
NOPE = 64
ROPE = 32
VH = 64
CW = 1024
KW = 3
TOK_DEV = 256
SEQ = 1024
SEQS = 4
N_TP = 2


def draw_q_gain(key, part):
    key = jax.random.fold_in(key, 11)
    return jnp.clip(1.0 + 0.18 * jax.random.normal(key, (QR,), jnp.float32), 0.3, 1.9)


def draw_kv_gain(key, part):
    key = jax.random.fold_in(key, 23)
    return jnp.clip(1.0 + 0.18 * jax.random.normal(key, (KVR,), jnp.float32), 0.3, 1.9)


def block_levels(key, extent, shards, smallest, high):
    level = 1.0
    for dim, parts in shards:
        steps = jax.random.uniform(jax.random.fold_in(jax.random.fold_in(key, 6), dim), (parts,), jnp.float32, smallest / len(shards), high / len(shards))
        level = level * jnp.repeat(jnp.exp(steps), extent[dim] // parts).reshape((-1,) + (1,) * (len(extent) - 1 - dim))
    return level


def normal_values(own_key, shape, deviation, reach, cuts=(), kind=jnp.bfloat16):
    array = jax.random.normal(own_key, shape, jnp.float32) * deviation
    if len(cuts) > 0:
        array = block_levels(own_key, shape, cuts, -0.22, 0.18) * array
    return jnp.clip(array, min=-reach, max=reach).astype(kind)


def setup_inputs(seed: int = 0) -> dict:
    key_list = jax.random.split(jax.random.key(seed), 17)
    tokens = normal_values(key_list[0], (SEQS, SEQ, D), 1.0, 6.0, ((0, 4), (1, 8)))
    h_gain = jnp.clip(1.0 + 0.18 * jax.random.normal(key_list[1], (D,), jnp.float32), 0.1, 1.9)
    w_qlat = normal_values(key_list[2], (D, QR), D ** -0.5, 0.125, ((0, 16),))
    w_kvlat = normal_values(key_list[3], (D, KVR), D ** -0.5, 0.125, ((0, 16),))
    w_krope = normal_values(key_list[4], (D, ROPE), D ** -0.5, 0.125, ((0, 16),))
    q_gain = draw_q_gain(jax.random.fold_in(key_list[16], 71), 0)
    kv_gain = draw_kv_gain(jax.random.fold_in(key_list[16], 71), 0)
    w_uq = normal_values(key_list[7], (QR, H * (NOPE + ROPE)), (QR // 3) ** -0.5, 0.375, ((1, 2),))
    w_uk = normal_values(key_list[8], (KVR, H * NOPE), (KVR // 3) ** -0.5, 0.4375, ((1, 2),))
    w_uv = normal_values(key_list[9], (KVR, H * VH), KVR ** -0.5, 0.25, ((1, 2),))
    w_convb = normal_values(key_list[10], (D, CW), D ** -0.5, 0.125, ((1, 2),))
    w_convc = normal_values(key_list[11], (D, CW), D ** -0.5, 0.125, ((1, 2),))
    w_convx = normal_values(key_list[12], (D, CW), D ** -0.5, 0.125, ((1, 2),))
    conv_taps = normal_values(key_list[13], (KW, CW), 0.58, 3.0, ((1, 2),), jnp.float32)
    w_out_attn = normal_values(key_list[14], (H * VH, D), (H * VH + CW) ** -0.5, 0.125, ((0, 2),))
    w_out_conv = normal_values(key_list[15], (CW, D), (H * VH + CW) ** -0.5, 0.125, ((0, 2),))
    return dict(tokens=tokens, h_gain=h_gain, w_qlat=w_qlat, w_kvlat=w_kvlat, w_krope=w_krope, q_gain=q_gain, kv_gain=kv_gain, w_uq=w_uq, w_uk=w_uk, w_uv=w_uv, w_convb=w_convb, w_convc=w_convc, w_convx=w_convx, conv_taps=conv_taps, w_out_attn=w_out_attn, w_out_conv=w_out_conv)


EPS = 1e-06
THETA = 10000.0

def normalize(values_in, gain):
    return values_in * lax.rsqrt(lax.optimization_barrier(jnp.mean(values_in * values_in, axis=-1, keepdims=True)) + EPS) * gain.astype(jnp.float32)

def angle_table(positions, dims):
    inverse = THETA ** (-jnp.arange(0, dims, 2, dtype=jnp.float32) / dims)
    return positions[:, None] * inverse

def rotate(values_in, angles):
    lower_half, upper_half = jnp.split(values_in, 2, axis=-1)
    cosine = jnp.cos(angles)
    sine_part = jnp.sin(angles)
    return jnp.concatenate([lower_half * cosine - upper_half * sine_part, lower_half * sine_part + upper_half * cosine], axis=-1)

def reference(tokens, h_gain, w_qlat, w_kvlat, w_krope, q_gain, kv_gain, w_uq, w_uk, w_uv, w_convb, w_convc, w_convx, conv_taps, w_out_attn, w_out_conv):
    score_scale = (NOPE + ROPE) ** (-0.5)
    blocks = SEQ // TOK_DEV
    head_width = H * VH // N_TP
    chan_width = CW // N_TP

    def one_sequence(rows_in):
        hidden = normalize(rows_in.astype(jnp.float32), h_gain).astype(jnp.bfloat16)
        query_norm = normalize(jnp.dot(hidden, w_qlat, preferred_element_type=jnp.float32), q_gain).astype(jnp.bfloat16)
        kv_norm = normalize(jnp.dot(hidden, w_kvlat, preferred_element_type=jnp.float32), kv_gain).astype(jnp.bfloat16)
        angles = angle_table(jnp.arange(SEQ, dtype=jnp.float32), ROPE)
        rope_key = rotate(jnp.dot(hidden, w_krope, preferred_element_type=jnp.float32), angles).astype(jnp.bfloat16)
        query = jnp.dot(query_norm, w_uq, preferred_element_type=jnp.float32).reshape(SEQ, H, NOPE + ROPE)
        query = jnp.concatenate([query[..., :NOPE], rotate(query[..., NOPE:], angles[:, None, :])], axis=-1).astype(jnp.bfloat16)
        key_nope = jnp.dot(kv_norm, w_uk, preferred_element_type=jnp.float32).astype(jnp.bfloat16).reshape(SEQ, H, NOPE)
        values = jnp.dot(kv_norm, w_uv, preferred_element_type=jnp.float32).astype(jnp.bfloat16).reshape(SEQ, H, VH)
        keys = jnp.concatenate([key_nope, jnp.broadcast_to(rope_key[:, None, :], (SEQ, H, ROPE))], axis=-1)

        def one_head(arrays):
            query_head, key_head, value_head = arrays

            def one_block(index):
                query_block = lax.dynamic_slice_in_dim(query_head, index * TOK_DEV, TOK_DEV, 0)
                scores = jnp.dot(query_block, key_head.T, preferred_element_type=jnp.float32) * score_scale
                query_pos = index * TOK_DEV + jnp.arange(TOK_DEV, dtype=jnp.int32)
                key_pos = jnp.arange(SEQ, dtype=jnp.int32)
                scores = jnp.where(key_pos[None, :] <= query_pos[:, None], scores, -jnp.inf)
                largest = lax.optimization_barrier(jnp.max(scores, axis=-1, keepdims=True))
                weights = jnp.exp(scores - largest)
                totals = lax.optimization_barrier(jnp.sum(weights, axis=-1, keepdims=True))
                return jnp.dot(weights.astype(jnp.bfloat16), value_head, preferred_element_type=jnp.float32) / totals
            return lax.map(one_block, jnp.arange(blocks, dtype=jnp.int32)).reshape(SEQ, VH)
        attn = lax.map(one_head, (query.transpose(1, 0, 2), keys.transpose(1, 0, 2), values.transpose(1, 0, 2)))
        attn = attn.transpose(1, 0, 2).reshape(SEQ, H * VH).astype(jnp.bfloat16)
        conv_b = jnp.dot(hidden, w_convb, preferred_element_type=jnp.float32)
        conv_c = jnp.dot(hidden, w_convc, preferred_element_type=jnp.float32)
        conv_x = jnp.dot(hidden, w_convx, preferred_element_type=jnp.float32)
        conv_in = (conv_c * conv_x).astype(jnp.bfloat16)
        padded = jnp.concatenate([jnp.zeros((KW - 1, CW), jnp.float32), conv_in.astype(jnp.float32)], axis=0)
        filtered = jnp.zeros((SEQ, CW), jnp.float32)
        for tap in range(KW):
            filtered = filtered + conv_taps[tap].astype(jnp.float32) * padded[tap:tap + SEQ]
        conv_out = (conv_b * filtered).astype(jnp.bfloat16)

        def add_group(summed, group):
            attn_part = lax.dynamic_slice_in_dim(attn, group * head_width, head_width, 1)
            attn_rows = lax.dynamic_slice_in_dim(w_out_attn, group * head_width, head_width, 0)
            conv_part = lax.dynamic_slice_in_dim(conv_out, group * chan_width, chan_width, 1)
            conv_rows = lax.dynamic_slice_in_dim(w_out_conv, group * chan_width, chan_width, 0)
            term = jnp.dot(attn_part, attn_rows, preferred_element_type=jnp.float32) + jnp.dot(conv_part, conv_rows, preferred_element_type=jnp.float32)
            rounded = lax.optimization_barrier(term.astype(jnp.bfloat16))
            return (summed + rounded.astype(jnp.float32), None)
        summed, _ = lax.scan(add_group, jnp.zeros((SEQ, D), jnp.float32), jnp.arange(N_TP, dtype=jnp.int32))
        return summed.astype(jnp.bfloat16)
    return lax.map(one_sequence, tokens)
```

```python
import functools

import jax
import jax.numpy as jnp
from jax import lax
from jax.experimental import pallas as pl
from jax.experimental.pallas import tpu as pltpu
from jax.sharding import PartitionSpec as P

NOPE = 64
ROPE = 32
VH = 64
KW = 3


EPS = 1e-06
THETA = 10000.0
NEG_START = -1e30


def from_behind(array, axis, by):
    size = lax.axis_size(axis)
    pairs = [(i, i + by) for i in range(size) if 0 <= i + by < size]
    return lax.ppermute(array, axis, pairs)


def normalize(values_in, gain):
    return (
        values_in * lax.rsqrt(jnp.mean(values_in * values_in, axis=-1, keepdims=True) + EPS) * gain
    )


def angle_table(positions, dims):
    inverse = THETA ** (-jnp.arange(0, dims, 2, dtype=jnp.float32) / dims)
    return positions[:, None] * inverse


def rotate(values_in, angles):
    lower_half, upper_half = jnp.split(values_in, 2, axis=-1)
    cosine = jnp.cos(angles)
    sine_part = jnp.sin(angles)
    return jnp.concatenate(
        [
            lower_half * cosine - upper_half * sine_part,
            lower_half * sine_part + upper_half * cosine,
        ],
        axis=-1,
    )


def per_device(
    tokens,
    h_gain,
    w_qlat,
    w_kvlat,
    w_krope,
    q_gain,
    kv_gain,
    w_uq,
    w_uk,
    w_uv,
    w_convb,
    w_convc,
    w_convx,
    conv_taps,
    w_out_attn,
    w_out_conv,
):
    own_rows = lax.all_gather(tokens, "tp", axis=1, tiled=True)
    seq_count = own_rows.shape[0]
    rows_here = own_rows.shape[1]
    flat_count = seq_count * rows_here
    hidden = normalize(own_rows.astype(jnp.float32), h_gain).astype(jnp.bfloat16)
    flat_hidden = hidden.reshape(flat_count, hidden.shape[2])
    groups = lax.axis_size("tp")
    member = lax.axis_index("tp")
    q_cols = w_qlat.shape[1] // groups
    kv_cols = w_kvlat.shape[1] // groups
    rope_cols = w_krope.shape[1] // groups
    q_part = lax.dynamic_slice_in_dim(w_qlat, member * q_cols, q_cols, 1)
    kv_part = lax.dynamic_slice_in_dim(w_kvlat, member * kv_cols, kv_cols, 1)
    rope_part = lax.dynamic_slice_in_dim(w_krope, member * rope_cols, rope_cols, 1)
    whole_q, whole_kv, whole_rope = (
        lax.all_gather(q_part, ("sp", "fs"), axis=0, tiled=True),
        lax.all_gather(kv_part, ("sp", "fs"), axis=0, tiled=True),
        lax.all_gather(rope_part, ("sp", "fs"), axis=0, tiled=True),
    )
    partial_latents = (
        jnp.dot(flat_hidden, whole_q, preferred_element_type=jnp.float32),
        jnp.dot(flat_hidden, whole_kv, preferred_element_type=jnp.float32),
        jnp.dot(flat_hidden, whole_rope, preferred_element_type=jnp.float32),
    )
    query_latent, kv_latent, rope_latent = (
        lax.all_gather(partial_latents[0], "tp", axis=1, tiled=True),
        lax.all_gather(partial_latents[1], "tp", axis=1, tiled=True),
        lax.all_gather(partial_latents[2], "tp", axis=1, tiled=True),
    )
    query_latent = query_latent.reshape(seq_count, rows_here, query_latent.shape[1])
    kv_latent = kv_latent.reshape(seq_count, rows_here, kv_latent.shape[1])
    rope_latent = rope_latent.reshape(seq_count, rows_here, rope_latent.shape[1])
    base = lax.axis_index("sp") * rows_here
    query_pos = base + jnp.arange(rows_here, dtype=jnp.int32)
    angles = angle_table(query_pos.astype(jnp.float32), ROPE)
    query_norm = normalize(query_latent, q_gain).astype(jnp.bfloat16)
    kv_norm = normalize(kv_latent, kv_gain).astype(jnp.bfloat16)
    rope_key = rotate(rope_latent, angles[None]).astype(jnp.bfloat16)
    head_count = w_uk.shape[1] // NOPE
    query = jnp.einsum("sqc,cn->sqn", query_norm, w_uq, preferred_element_type=jnp.float32).reshape(
        seq_count, rows_here, head_count, NOPE + ROPE
    )
    query = jnp.concatenate(
        [query[..., :NOPE], rotate(query[..., NOPE:], angles[None, :, None, :])], axis=-1
    ).astype(jnp.bfloat16)
    query = query.transpose(0, 2, 1, 3)
    score_scale = (NOPE + ROPE) ** (-0.5)
    last_query = base + rows_here - 1
    fold_start = (
        jnp.full((seq_count, head_count, rows_here), NEG_START, jnp.float32),
        jnp.zeros((seq_count, head_count, rows_here), jnp.float32),
        jnp.zeros((seq_count, head_count, rows_here, VH), jnp.float32),
    )
    pieces = (
        lax.all_gather(kv_norm, "sp", axis=1, tiled=True),
        lax.all_gather(rope_key, "sp", axis=1, tiled=True),
    )

    def make_keys():
        key_nope = jnp.einsum(
            "skc,cn->skn", pieces[0], w_uk, preferred_element_type=jnp.float32
        ).astype(jnp.bfloat16)
        value_rows = jnp.einsum(
            "skc,cn->skn", pieces[0], w_uv, preferred_element_type=jnp.float32
        ).astype(jnp.bfloat16)
        return (key_nope, value_rows, pieces[1])

    def compute(state):
        running_max, running_sum, weighted = state
        key_nope, value_rows, rope_piece = make_keys()
        width = rope_piece.shape[1]
        keys = jnp.concatenate(
            [
                key_nope.reshape(seq_count, width, head_count, NOPE),
                jnp.broadcast_to(rope_piece[:, :, None, :], (seq_count, width, head_count, ROPE)),
            ],
            axis=-1,
        )
        scores = (
            jnp.einsum("shqd,skhd->shqk", query, keys, preferred_element_type=jnp.float32)
            * score_scale
        )
        key_pos = jnp.arange(width, dtype=jnp.int32)
        visible = key_pos[None, :] <= query_pos[:, None]
        scores = jnp.where(visible[None, None], scores, -jnp.inf)
        new_max = jnp.maximum(running_max, jnp.max(scores, axis=-1))
        weights = jnp.exp(scores - new_max[..., None])
        new_sum = jnp.sum(weights, axis=-1)
        update = jnp.einsum(
            "shqk,skhv->shqv",
            weights.astype(jnp.bfloat16),
            value_rows.reshape(seq_count, width, head_count, VH),
            preferred_element_type=jnp.float32,
        )
        return (new_max, new_sum, update)

    def keep(state):
        return state

    final = lax.cond(jnp.int32(0) <= last_query, compute, keep, fold_start)
    attn = (
        (final[2] / final[1][..., None])
        .transpose(0, 2, 1, 3)
        .reshape(seq_count, rows_here, head_count * VH)
        .astype(jnp.bfloat16)
    )
    conv_b = jnp.dot(flat_hidden, w_convb, preferred_element_type=jnp.float32).reshape(
        seq_count, rows_here, w_convb.shape[1]
    )
    conv_c = jnp.dot(flat_hidden, w_convc, preferred_element_type=jnp.float32)
    conv_x = jnp.dot(flat_hidden, w_convx, preferred_element_type=jnp.float32)
    conv_in = (conv_c * conv_x).astype(jnp.bfloat16).reshape(seq_count, rows_here, w_convc.shape[1])
    edge_rows = from_behind(conv_in[:, rows_here - (KW - 1) :], "sp", 1)
    padded = jnp.concatenate([edge_rows, conv_in], axis=1).astype(jnp.float32)
    filtered = jnp.zeros(conv_b.shape, jnp.float32)
    for tap in range(KW):
        filtered = filtered + conv_taps[tap] * padded[:, tap : tap + rows_here]
    conv_out = (conv_b * filtered).astype(jnp.bfloat16)
    result = lax.psum_scatter(
        (
            jnp.einsum("sqc,cd->qsd", attn, w_out_attn, preferred_element_type=jnp.float32)
            + jnp.einsum("sqc,cd->qsd", conv_out, w_out_conv, preferred_element_type=jnp.float32)
        ).astype(jnp.bfloat16),
        "tp",
        scatter_dimension=0,
        tiled=True,
    )
    return result.transpose(1, 0, 2)


MESH = pl.DeviceIdType.MESH
F32 = jnp.float32
BF16 = jnp.bfloat16
KV, RK, QL = 0, 1, 2


def dot(a, b):
    return jnp.dot(a, b, preferred_element_type=F32)


def dot_t(a, b):
    return lax.dot_general(a, b, (((1,), (1,)), ((), ())), preferred_element_type=F32)


def fused_kernel(
    ns, nf,
    tok, h_gain, wq, wkv, wr, q_gain, kv_gain, taps, cos_t, sin_t, cos_q, sin_q,
    wb_hbm, wc_hbm, wx_hbm, wuq_hbm, wuk_hbm, wuv_hbm, woa_hbm, woc_hbm,
    out,
    tok_in, hid, wq_buf, wkv_buf, wr_buf, wb, wc, wx, wuq, wuk, wuv, woa, woc,
    cbuf, tail_out, tail_in, conv_out,
    lat_kv, lat_q, kvn, rk, k_buf, v_buf, q_buf, a_buf, part, part_in,
    load_sem, send_sem, recv_sem, half_sem, tp_send, tp_recv, kz_send, kz_recv, kt_send, kt_recv,
    tail_sem, out_send, out_recv,
):
    z, f, m = lax.axis_index("sp"), lax.axis_index("fs"), lax.axis_index("tp")
    fx = f + 1 - 2 * (f % 2)
    fy = (f + 2) % 4
    fd = fx + 2 - 4 * (fx // 2)
    other = 1 - m
    to_x, to_y, to_tp = {"fs": fx}, {"fs": fy}, {"tp": other}
    to_right, to_left = {"sp": z + 1}, {"sp": z - 1}
    half_rows, rows = tok.shape[0], hid.shape[0]
    has_right, has_left = z < ns - 1, z > 0
    bufs = (wkv_buf, wr_buf, wq_buf)
    kv_w, q_w = wkv_buf.shape[2], wq_buf.shape[2]
    kv_own = wkv.at[:, pl.ds(pl.multiple_of(m * kv_w, kv_w), kv_w)]
    q_own = wq.at[:, pl.ds(pl.multiple_of(m * q_w, q_w), q_w)]
    owns = (kv_own, wr, q_own)
    me = z * nf + f

    barrier = pltpu.get_barrier_semaphore()
    for target in (to_x, to_y, to_tp):
        pl.semaphore_signal(barrier, inc=1, device_id=target, device_id_type=MESH)

    @pl.when(has_right)
    def _():
        pl.semaphore_signal(barrier, inc=1, device_id=to_right, device_id_type=MESH)

    @pl.when(has_left)
    def _():
        pl.semaphore_signal(barrier, inc=1, device_id=to_left, device_id_type=MESH)

    loads = [
        pltpu.make_async_copy(a, b, load_sem.at[i])
        for i, (a, b) in enumerate(
            ((wc_hbm, wc), (wx_hbm, wx), (wb_hbm, wb), (wuk_hbm, wuk), (wuv_hbm, wuv),
             (wuq_hbm, wuq), (woa_hbm, woa), (woc_hbm, woc))
        )
    ]
    for load in loads:
        load.start()
    pl.semaphore_wait(barrier, 3 + jnp.where(has_right, 1, 0) + jnp.where(has_left, 1, 0))

    def remote(src, dst, send, recv, target):
        return pltpu.make_async_remote_copy(
            src_ref=src, dst_ref=dst, send_sem=send, recv_sem=recv,
            device_id=target, device_id_type=MESH,
        )

    def whole(kind, src, slot, lane, target):
        return remote(
            src, bufs[kind].at[slot], send_sem.at[kind, slot, lane], recv_sem.at[kind, slot], target
        )

    def half_of(kind, which):
        size = bufs[kind].shape[1] // 2
        return pl.ds(which * size, size)

    def half(kind, slot, which, target):
        place = bufs[kind].at[slot, half_of(kind, which)]
        return remote(
            place, place, send_sem.at[kind, slot, which], half_sem.at[kind, slot, which], target
        )

    def send_on(kinds, slot, left, right, own=False):
        for kind in kinds:
            src = owns[kind] if own else bufs[kind].at[slot]
            if right is not None:
                @pl.when(right)
                def _(kind=kind, src=src):
                    whole(kind, src, slot, 2, to_right).start()
            if left is not None:
                @pl.when(left)
                def _(kind=kind, src=src):
                    whole(kind, src, slot, 3, to_left).start()
            whole(kind, src, slot, 0, to_x).start()
            whole(kind, src, slot, 1, to_y).start()

    def arrive(kinds, slot):
        for kind in kinds:
            whole(kind, bufs[kind].at[slot], slot, 0, to_x).wait_recv()

    def z_step(kinds, d):
        @pl.when(z - d >= 0)
        def _():
            slot = (z - d) * nf + f
            arrive(kinds, slot)
            send_on(kinds, slot, None, has_right)

        @pl.when(z + d < ns)
        def _():
            slot = (z + d) * nf + f
            arrive(kinds, slot)
            send_on(kinds, slot, has_left, None)

    def diag_at(kinds, zo):
        arrive(kinds, zo * nf + fx)
        for kind in kinds:
            half(kind, zo * nf + fx, 0, to_y).start()
        arrive(kinds, zo * nf + fy)
        for kind in kinds:
            half(kind, zo * nf + fy, 1, to_x).start()

    def diag_step(kinds, d):
        if d == 0:
            diag_at(kinds, z)
            return

        @pl.when(z - d >= 0)
        def _():
            diag_at(kinds, z - d)

        @pl.when(z + d < ns)
        def _():
            diag_at(kinds, z + d)

    def diag_done(kinds):
        for zo in range(ns):
            for kind in kinds:
                for which in range(2):
                    half(kind, zo * nf + fd, which, to_x).wait_recv()

    first, second = (KV, RK), (QL,)
    tok_copy = remote(tok, tok_in, tp_send.at[0], tp_recv.at[0], to_tp)
    tok_copy.start()
    send_on(first, me, has_left, has_right, own=True)
    wkv_buf[me] = kv_own[...]
    wr_buf[me] = wr[...]
    wq_buf[me] = q_own[...]

    def norm_rows(src, block):
        data = src[...].astype(F32)
        hid[pl.ds(pl.multiple_of(block * half_rows, half_rows), half_rows)] = normalize(
            data, h_gain[...]
        ).astype(BF16)

    norm_rows(tok, m)
    tok_copy.wait()
    norm_rows(tok_in, other)
    z_step(first, 1)

    width = 256
    tiles = wc.shape[1] // width
    pad = 8

    def conv_tile(t, carry):
        cols = pl.ds(pl.multiple_of(t * width, width), width)
        made = (dot(hid[...], wc[:, cols]) * dot(hid[...], wx[:, cols])).astype(BF16)
        cbuf[pl.ds(pad, rows), cols] = made.astype(F32)
        tail_out[:, cols] = made[rows - tail_out.shape[0] :]
        return carry

    loads[0].wait()
    loads[1].wait()
    diag_step(first, 0)
    conv_tile(0, 0)
    z_step(first, 2)
    diag_step(first, 1)
    lax.fori_loop(1, tiles, conv_tile, 0)
    tail_copy = remote(tail_out, tail_in, tail_sem.at[0], tail_sem.at[1], to_right)

    @pl.when(has_right)
    def _():
        tail_copy.start()

    for d in range(3, ns):
        z_step(first, d)
        diag_step(first, d - 1)
    send_on(second, me, has_left, has_right, own=True)
    diag_step(first, ns - 1)
    z_step(second, 1)
    diag_step(second, 0)

    @pl.when(has_left)
    def _():
        tail_copy.wait_recv()
        cbuf[0:pad] = tail_in[tail_in.shape[0] - pad :].astype(F32)

    @pl.when(jnp.logical_not(has_left))
    def _():
        cbuf[0:pad] = jnp.zeros((pad, cbuf.shape[1]), F32)

    loads[2].wait()

    def gate_tile(t, carry):
        cols = pl.ds(pl.multiple_of(t * width, width), width)
        gate = dot(hid[...], wb[:, cols])
        filtered = jnp.zeros((rows, width), F32)
        for tap in range(KW):
            start = pad - (KW - 1) + tap
            filtered = filtered + taps[tap : tap + 1, cols] * cbuf[pl.ds(start, rows), cols]
        conv_out[:, cols] = (gate * filtered).astype(BF16)
        return carry

    lax.fori_loop(0, tiles, gate_tile, 0)
    z_step(second, 2)
    diag_step(second, 1)

    diag_done(first)
    depth = hid.shape[1]
    lat_kv[m] = dot(hid[...], wkv_buf[...].reshape(depth, kv_w))
    kv_copy = remote(lat_kv.at[m], lat_kv.at[m], tp_send.at[1], tp_recv.at[1], to_tp)
    kv_copy.start()
    w_rope = jnp.concatenate([wr_buf[s] for s in range(ns * nf)], axis=1)
    rope = dot_t(w_rope, hid[...])
    low, high = rope[: ROPE // 2], rope[ROPE // 2 :]
    cos_v, sin_v = cos_t[...], sin_t[...]
    rk[z] = jnp.concatenate(
        [low * cos_v - high * sin_v, low * sin_v + high * cos_v], axis=0
    ).astype(BF16)
    for d in range(3, ns):
        z_step(second, d)
        diag_step(second, d - 1)

    def latent_norm(lat, gain):
        left, right = lat[0], lat[1]
        mean = (
            jnp.sum(left * left, axis=-1, keepdims=True)
            + jnp.sum(right * right, axis=-1, keepdims=True)
        ) / (2 * left.shape[1])
        scale = lax.rsqrt(mean + EPS)
        cut = left.shape[1]
        return (
            (left * scale * gain[:, :cut]).astype(BF16),
            (right * scale * gain[:, cut:]).astype(BF16),
        )

    kv_copy.wait()
    left, right = latent_norm(lat_kv, kv_gain[...])
    kvn[z, 0] = left
    kvn[z, 1] = right

    def pass_right(origin):
        remote(kvn.at[origin, m], kvn.at[origin, m], kz_send.at[0, origin], kz_recv.at[0, origin], to_right).start()
        remote(rk.at[origin], rk.at[origin], kz_send.at[1, origin], kz_recv.at[1, origin], to_right).start()

    def kz(which, origin):
        ref = kvn.at[origin, m] if which == 0 else rk.at[origin]
        return remote(ref, ref, kz_send.at[which, origin], kz_recv.at[which, origin], to_right)

    def kt(origin, part_of):
        ref = kvn.at[origin, part_of]
        return remote(ref, ref, kt_send.at[origin], kt_recv.at[origin], to_tp)

    @pl.when(has_right)
    def _():
        pass_right(z)

    loads[3].wait()
    loads[4].wait()

    def make_keys(origin):
        lhs = jnp.concatenate([kvn[origin, 0], kvn[origin, 1]], axis=1)
        place = pl.ds(pl.multiple_of(origin * rows, rows), rows)

        def pair(p, carry):
            cols = pl.ds(pl.multiple_of(p * width, width), width)
            keys = dot(lhs, wuk[:, cols]).astype(BF16)
            vals = dot(lhs, wuv[:, cols]).astype(BF16)
            for i in range(2):
                k_buf[2 * p + i, place] = keys[:, 128 * i : 128 * (i + 1)]
                v_buf[2 * p + i, place] = vals[:, 128 * i : 128 * (i + 1)]
            return carry

        lax.fori_loop(0, wuk.shape[1] // width, pair, 0)

    make_keys(z)
    for d in range(1, ns):
        @pl.when(z + d < ns)
        def _(d=d):
            place = pl.ds(pl.multiple_of((z + d) * rows, rows), rows)
            k_buf[:, place] = jnp.zeros((k_buf.shape[0], rows, 128), BF16)
            v_buf[:, place] = jnp.zeros((v_buf.shape[0], rows, 128), BF16)
            rk[z + d] = jnp.zeros(rk.shape[1:], BF16)

    diag_step(second, ns - 1)

    def take_keys(d):
        @pl.when(z - d >= 0)
        def _():
            origin = z - d
            kz(0, origin).wait_recv()
            kz(1, origin).wait_recv()
            kt(origin, m).start()

            @pl.when(has_right)
            def _():
                pass_right(origin)

    def use_keys(d):
        @pl.when(z - d >= 0)
        def _():
            kt(z - d, other).wait_recv()
            make_keys(z - d)

    for d in range(1, ns):
        take_keys(d)
        if d > 1:
            use_keys(d - 1)
    diag_done(second)
    lat_q[m] = dot(hid[...], wq_buf[...].reshape(depth, q_w))
    q_copy = remote(lat_q.at[m], lat_q.at[m], tp_send.at[2], tp_recv.at[2], to_tp)
    q_copy.start()
    use_keys(ns - 1)
    q_copy.wait()
    q_left, q_right = latent_norm(lat_q, q_gain[...])
    q_norm = jnp.concatenate([q_left, q_right], axis=1)
    loads[5].wait()
    head = NOPE + ROPE
    heads = wuq.shape[1] // head
    query = dot(q_norm, wuq[...])
    cos_r, sin_r = cos_q[...], sin_q[...]
    for h in range(heads):
        one = query[:, h * head : (h + 1) * head]
        low, high = one[:, NOPE : NOPE + ROPE // 2], one[:, NOPE + ROPE // 2 :]
        q_buf[h] = jnp.concatenate(
            [one[:, :NOPE], low * cos_r - high * sin_r, low * sin_r + high * cos_r], axis=1
        ).astype(BF16)

    rope_keys = jnp.concatenate([rk[s] for s in range(ns)], axis=1)
    span = ns * rows
    visible = lax.broadcasted_iota(jnp.int32, (rows, span), 1) <= (
        z * rows + lax.broadcasted_iota(jnp.int32, (rows, span), 0)
    )

    def attend(p, carry):
        done = []
        for i in range(2):
            qh = q_buf[2 * p + i]
            kh = k_buf[p][:, NOPE * i : NOPE * (i + 1)]
            vh = v_buf[p][:, VH * i : VH * (i + 1)]
            scores = dot_t(qh[:, :NOPE], kh) + dot(qh[:, NOPE:], rope_keys)
            scores = jnp.where(visible, scores * head ** (-0.5), -jnp.inf)
            weights = jnp.exp(scores - jnp.max(scores, axis=-1, keepdims=True))
            total = jnp.sum(weights, axis=-1, keepdims=True)
            done.append(dot(weights.astype(BF16), vh) / total)
        a_buf[p] = jnp.concatenate(done, axis=1).astype(BF16)
        return carry

    lax.fori_loop(0, heads // 2, attend, 0)
    attn = jnp.concatenate([a_buf[p] for p in range(heads // 2)], axis=1)
    loads[6].wait()
    loads[7].wait()
    step = 512

    def out_copy(t):
        cols = pl.ds(pl.multiple_of(t * step, step), step)
        return remote(
            part.at[other, :, cols], part_in.at[:, cols], out_send.at[t], out_recv.at[t], to_tp
        )

    def project(t, carry):
        cols = pl.ds(pl.multiple_of(t * step, step), step)
        term = (dot(attn, woa[:, cols]) + dot(conv_out[...], woc[:, cols])).astype(BF16)
        part[0, :, cols] = term[:half_rows]
        part[1, :, cols] = term[half_rows:]
        out_copy(t).start()
        return carry

    count = out.shape[1] // step
    lax.fori_loop(0, count, project, 0)

    def finish(t, carry):
        cols = pl.ds(pl.multiple_of(t * step, step), step)
        out_copy(t).wait_recv()
        out[:, cols] = (part[m, :, cols].astype(F32) + part_in[:, cols].astype(F32)).astype(BF16)
        return carry

    lax.fori_loop(0, count, finish, 0)

    def sent_slot(kind, slot, left, right):
        ref = bufs[kind].at[slot]
        if right is not None:
            @pl.when(right)
            def _():
                whole(kind, ref, slot, 2, to_right).wait_send()
        if left is not None:
            @pl.when(left)
            def _():
                whole(kind, ref, slot, 3, to_left).wait_send()
        whole(kind, ref, slot, 0, to_x).wait_send()
        whole(kind, ref, slot, 1, to_y).wait_send()

    for kind in (KV, RK, QL):
        sent_slot(kind, me, has_left, has_right)
        for d in range(1, ns):
            @pl.when(z - d >= 0)
            def _(d=d, kind=kind):
                sent_slot(kind, (z - d) * nf + f, None, has_right)

            @pl.when(z + d < ns)
            def _(d=d, kind=kind):
                sent_slot(kind, (z + d) * nf + f, has_left, None)
        for zo in range(ns):
            half(kind, zo * nf + fx, 0, to_y).wait_send()
            half(kind, zo * nf + fy, 1, to_x).wait_send()

    @pl.when(has_right)
    def _():
        tail_copy.wait_send()
        for d in range(ns):
            @pl.when(z - d >= 0)
            def _(d=d):
                kz(0, z - d).wait_send()
                kz(1, z - d).wait_send()

    for d in range(1, ns):
        @pl.when(z - d >= 0)
        def _(d=d):
            kt(z - d, m).wait_send()

    def sent_out(t, carry):
        out_copy(t).wait_send()
        return carry

    lax.fori_loop(0, count, sent_out, 0)


def fused_device(
    ns, nf, tokens, h_gain, w_qlat, w_kvlat, w_krope, q_gain, kv_gain, w_uq, w_uk, w_uv,
    w_convb, w_convc, w_convx, conv_taps, w_out_attn, w_out_conv,
):
    half_rows, depth = tokens.shape[1:]
    rows = 2 * half_rows
    slots = ns * nf
    cut = w_qlat.shape[0]
    heads = w_uk.shape[1] // NOPE
    positions = (lax.axis_index("sp") * rows + jnp.arange(rows, dtype=jnp.int32)).astype(F32)
    angles = angle_table(positions, ROPE)
    cos_q, sin_q = jnp.cos(angles), jnp.sin(angles)
    vmem = pl.BlockSpec(memory_space=pltpu.VMEM)
    anywhere = pl.BlockSpec(memory_space=pl.ANY)
    V, DMA = pltpu.VMEM, pltpu.SemaphoreType.DMA
    big = (w_convb, w_convc, w_convx, w_uq, w_uk, w_uv, w_out_attn, w_out_conv)
    span = ns * rows
    q_w, kv_w = w_qlat.shape[1] // 2, w_kvlat.shape[1] // 2
    result = pl.pallas_call(
        functools.partial(fused_kernel, ns, nf),
        out_shape=jax.ShapeDtypeStruct((half_rows, depth), BF16),
        in_specs=[vmem] * 12 + [anywhere] * 8,
        out_specs=vmem,
        scratch_shapes=[
            V((half_rows, depth), BF16), V((rows, depth), BF16),
            V((slots, cut, q_w), BF16), V((slots, cut, kv_w), BF16), V((slots, ROPE, cut), BF16),
        ] + [V(w.shape, BF16) for w in big] + [
            V((rows + 8, w_convc.shape[1]), F32),
            V((16, w_convc.shape[1]), BF16), V((16, w_convc.shape[1]), BF16),
            V((rows, w_convc.shape[1]), BF16),
            V((2, rows, kv_w), F32), V((2, rows, q_w), F32),
            V((ns, 2, rows, kv_w), BF16), V((ns, ROPE, rows), BF16),
            V((heads // 2, span, 2 * NOPE), BF16), V((heads // 2, span, 2 * VH), BF16),
            V((heads, rows, NOPE + ROPE), BF16), V((heads // 2, rows, 2 * VH), BF16),
            V((2, half_rows, depth), BF16), V((half_rows, depth), BF16),
            DMA((8,)), DMA((3, slots, 4)), DMA((3, slots)), DMA((3, slots, 2)),
            DMA((3,)), DMA((3,)), DMA((2, ns)), DMA((2, ns)), DMA((ns,)), DMA((ns,)),
            DMA((2,)), DMA((4,)), DMA((4,)),
        ],
        compiler_params=pltpu.CompilerParams(
            collective_id=0, has_side_effects=True, vmem_limit_bytes=60 * 1024 * 1024
        ),
    )(
        tokens[0], h_gain[None], w_qlat, w_kvlat, w_krope.T, q_gain[None], kv_gain[None],
        conv_taps, cos_q.T, sin_q.T, cos_q, sin_q, *big,
    )
    return result[None]


def solution(mesh):
    in_specs = (
        P("fs", ("sp", "tp"), None),
        P(),
        P(("sp", "fs"), None),
        P(("sp", "fs"), None),
        P(("sp", "fs"), None),
        P(),
        P(),
        P(None, "tp"),
        P(None, "tp"),
        P(None, "tp"),
        P(None, "tp"),
        P(None, "tp"),
        P(None, "tp"),
        P(None, "tp"),
        P("tp", None),
        P("tp", None),
    )
    out_specs = P("fs", ("sp", "tp"), None)
    fits = mesh.shape["tp"] == 2 and mesh.shape["fs"] == 4
    body = functools.partial(fused_device, mesh.shape["sp"], mesh.shape["fs"]) if fits else per_device
    return jax.shard_map(
        body, mesh=mesh, in_specs=in_specs, out_specs=out_specs, check_vma=False
    )
```

```python
import functools

import jax
import jax.numpy as jnp
from jax import lax
from jax.experimental import pallas as pl
from jax.experimental.pallas import tpu as pltpu
from jax.sharding import PartitionSpec as P

NOPE = 64
ROPE = 32
VH = 64
KW = 3


EPS = 1e-06
THETA = 10000.0
NEG_START = -1e30


def from_behind(array, axis, by):
    size = lax.axis_size(axis)
    pairs = [(i, i + by) for i in range(size) if 0 <= i + by < size]
    return lax.ppermute(array, axis, pairs)


def normalize(values_in, gain):
    return (
        values_in * lax.rsqrt(jnp.mean(values_in * values_in, axis=-1, keepdims=True) + EPS) * gain
    )


def angle_table(positions, dims):
    inverse = THETA ** (-jnp.arange(0, dims, 2, dtype=jnp.float32) / dims)
    return positions[:, None] * inverse


def rotate(values_in, angles):
    lower_half, upper_half = jnp.split(values_in, 2, axis=-1)
    cosine = jnp.cos(angles)
    sine_part = jnp.sin(angles)
    return jnp.concatenate(
        [
            lower_half * cosine - upper_half * sine_part,
            lower_half * sine_part + upper_half * cosine,
        ],
        axis=-1,
    )


def per_device(
    tokens,
    h_gain,
    w_qlat,
    w_kvlat,
    w_krope,
    q_gain,
    kv_gain,
    w_uq,
    w_uk,
    w_uv,
    w_convb,
    w_convc,
    w_convx,
    conv_taps,
    w_out_attn,
    w_out_conv,
):
    own_rows = lax.all_gather(tokens, "tp", axis=1, tiled=True)
    seq_count = own_rows.shape[0]
    rows_here = own_rows.shape[1]
    flat_count = seq_count * rows_here
    hidden = normalize(own_rows.astype(jnp.float32), h_gain).astype(jnp.bfloat16)
    flat_hidden = hidden.reshape(flat_count, hidden.shape[2])
    groups = lax.axis_size("tp")
    member = lax.axis_index("tp")
    q_cols = w_qlat.shape[1] // groups
    kv_cols = w_kvlat.shape[1] // groups
    rope_cols = w_krope.shape[1] // groups
    q_part = lax.dynamic_slice_in_dim(w_qlat, member * q_cols, q_cols, 1)
    kv_part = lax.dynamic_slice_in_dim(w_kvlat, member * kv_cols, kv_cols, 1)
    rope_part = lax.dynamic_slice_in_dim(w_krope, member * rope_cols, rope_cols, 1)
    whole_q, whole_kv, whole_rope = (
        lax.all_gather(q_part, ("sp", "fs"), axis=0, tiled=True),
        lax.all_gather(kv_part, ("sp", "fs"), axis=0, tiled=True),
        lax.all_gather(rope_part, ("sp", "fs"), axis=0, tiled=True),
    )
    partial_latents = (
        jnp.dot(flat_hidden, whole_q, preferred_element_type=jnp.float32),
        jnp.dot(flat_hidden, whole_kv, preferred_element_type=jnp.float32),
        jnp.dot(flat_hidden, whole_rope, preferred_element_type=jnp.float32),
    )
    query_latent, kv_latent, rope_latent = (
        lax.all_gather(partial_latents[0], "tp", axis=1, tiled=True),
        lax.all_gather(partial_latents[1], "tp", axis=1, tiled=True),
        lax.all_gather(partial_latents[2], "tp", axis=1, tiled=True),
    )
    query_latent = query_latent.reshape(seq_count, rows_here, query_latent.shape[1])
    kv_latent = kv_latent.reshape(seq_count, rows_here, kv_latent.shape[1])
    rope_latent = rope_latent.reshape(seq_count, rows_here, rope_latent.shape[1])
    base = lax.axis_index("sp") * rows_here
    query_pos = base + jnp.arange(rows_here, dtype=jnp.int32)
    angles = angle_table(query_pos.astype(jnp.float32), ROPE)
    query_norm = normalize(query_latent, q_gain).astype(jnp.bfloat16)
    kv_norm = normalize(kv_latent, kv_gain).astype(jnp.bfloat16)
    rope_key = rotate(rope_latent, angles[None]).astype(jnp.bfloat16)
    head_count = w_uk.shape[1] // NOPE
    query = jnp.einsum("sqc,cn->sqn", query_norm, w_uq, preferred_element_type=jnp.float32).reshape(
        seq_count, rows_here, head_count, NOPE + ROPE
    )
    query = jnp.concatenate(
        [query[..., :NOPE], rotate(query[..., NOPE:], angles[None, :, None, :])], axis=-1
    ).astype(jnp.bfloat16)
    query = query.transpose(0, 2, 1, 3)
    score_scale = (NOPE + ROPE) ** (-0.5)
    last_query = base + rows_here - 1
    fold_start = (
        jnp.full((seq_count, head_count, rows_here), NEG_START, jnp.float32),
        jnp.zeros((seq_count, head_count, rows_here), jnp.float32),
        jnp.zeros((seq_count, head_count, rows_here, VH), jnp.float32),
    )
    pieces = (
        lax.all_gather(kv_norm, "sp", axis=1, tiled=True),
        lax.all_gather(rope_key, "sp", axis=1, tiled=True),
    )

    def make_keys():
        key_nope = jnp.einsum(
            "skc,cn->skn", pieces[0], w_uk, preferred_element_type=jnp.float32
        ).astype(jnp.bfloat16)
        value_rows = jnp.einsum(
            "skc,cn->skn", pieces[0], w_uv, preferred_element_type=jnp.float32
        ).astype(jnp.bfloat16)
        return (key_nope, value_rows, pieces[1])

    def compute(state):
        running_max, running_sum, weighted = state
        key_nope, value_rows, rope_piece = make_keys()
        width = rope_piece.shape[1]
        keys = jnp.concatenate(
            [
                key_nope.reshape(seq_count, width, head_count, NOPE),
                jnp.broadcast_to(rope_piece[:, :, None, :], (seq_count, width, head_count, ROPE)),
            ],
            axis=-1,
        )
        scores = (
            jnp.einsum("shqd,skhd->shqk", query, keys, preferred_element_type=jnp.float32)
            * score_scale
        )
        key_pos = jnp.arange(width, dtype=jnp.int32)
        visible = key_pos[None, :] <= query_pos[:, None]
        scores = jnp.where(visible[None, None], scores, -jnp.inf)
        new_max = jnp.maximum(running_max, jnp.max(scores, axis=-1))
        weights = jnp.exp(scores - new_max[..., None])
        new_sum = jnp.sum(weights, axis=-1)
        update = jnp.einsum(
            "shqk,skhv->shqv",
            weights.astype(jnp.bfloat16),
            value_rows.reshape(seq_count, width, head_count, VH),
            preferred_element_type=jnp.float32,
        )
        return (new_max, new_sum, update)

    def keep(state):
        return state

    final = lax.cond(jnp.int32(0) <= last_query, compute, keep, fold_start)
    attn = (
        (final[2] / final[1][..., None])
        .transpose(0, 2, 1, 3)
        .reshape(seq_count, rows_here, head_count * VH)
        .astype(jnp.bfloat16)
    )
    conv_b = jnp.dot(flat_hidden, w_convb, preferred_element_type=jnp.float32).reshape(
        seq_count, rows_here, w_convb.shape[1]
    )
    conv_c = jnp.dot(flat_hidden, w_convc, preferred_element_type=jnp.float32)
    conv_x = jnp.dot(flat_hidden, w_convx, preferred_element_type=jnp.float32)
    conv_in = (conv_c * conv_x).astype(jnp.bfloat16).reshape(seq_count, rows_here, w_convc.shape[1])
    edge_rows = from_behind(conv_in[:, rows_here - (KW - 1) :], "sp", 1)
    padded = jnp.concatenate([edge_rows, conv_in], axis=1).astype(jnp.float32)
    filtered = jnp.zeros(conv_b.shape, jnp.float32)
    for tap in range(KW):
        filtered = filtered + conv_taps[tap] * padded[:, tap : tap + rows_here]
    conv_out = (conv_b * filtered).astype(jnp.bfloat16)
    result = lax.psum_scatter(
        (
            jnp.einsum("sqc,cd->qsd", attn, w_out_attn, preferred_element_type=jnp.float32)
            + jnp.einsum("sqc,cd->qsd", conv_out, w_out_conv, preferred_element_type=jnp.float32)
        ).astype(jnp.bfloat16),
        "tp",
        scatter_dimension=0,
        tiled=True,
    )
    return result.transpose(1, 0, 2)


MESH = pl.DeviceIdType.MESH
F32 = jnp.float32
BF16 = jnp.bfloat16
KV, RK, QL = 0, 1, 2


def dot(a, b):
    return jnp.dot(a, b, preferred_element_type=F32)


def dot_t(a, b):
    return lax.dot_general(a, b, (((1,), (1,)), ((), ())), preferred_element_type=F32)


def fused_kernel(
    ns, nf,
    tok, h_gain, wq, wkv, wr, q_gain, kv_gain, taps, inverse,
    wb_hbm, wc_hbm, wx_hbm, wuq_hbm, wuk_hbm, wuv_hbm, woa_hbm, woc_hbm,
    out,
    tok_in, hid, wq_buf, wkv_buf, wr_buf, wb, wc, wx, wuq, wuk, wuv, woa, woc,
    cbuf, tail_out, tail_in, conv_out,
    lat_kv, lat_q, kvn, rk, k_buf, rk_buf, v_buf, wn, wp, cos_r, sin_r, q_rope, q_buf, a_buf, part, part_in,
    load_sem, send_sem, recv_sem, half_sem, tp_send, tp_recv, kz_send, kz_recv, kt_send, kt_recv,
    tail_sem, out_send, out_recv,
):
    z, f, m = lax.axis_index("sp"), lax.axis_index("fs"), lax.axis_index("tp")
    fx = f + 1 - 2 * (f % 2)
    fy = (f + 2) % 4
    fd = fx + 2 - 4 * (fx // 2)
    other = 1 - m
    to_x, to_y, to_tp = {"fs": fx}, {"fs": fy}, {"tp": other}
    to_right, to_left = {"sp": z + 1}, {"sp": z - 1}
    half_rows, rows = tok.shape[0], hid.shape[0]
    has_right, has_left = z < ns - 1, z > 0
    bufs = (wkv_buf, wr_buf, wq_buf)
    kv_w, q_w = wkv_buf.shape[2], wq_buf.shape[2]
    kv_own = wkv.at[:, pl.ds(pl.multiple_of(m * kv_w, kv_w), kv_w)]
    q_own = wq.at[:, pl.ds(pl.multiple_of(m * q_w, q_w), q_w)]
    owns = (kv_own, wr, q_own)
    me = z * nf + f

    barrier = pltpu.get_barrier_semaphore()
    for target in (to_x, to_y, to_tp):
        pl.semaphore_signal(barrier, inc=1, device_id=target, device_id_type=MESH)

    @pl.when(has_right)
    def _():
        pl.semaphore_signal(barrier, inc=1, device_id=to_right, device_id_type=MESH)

    @pl.when(has_left)
    def _():
        pl.semaphore_signal(barrier, inc=1, device_id=to_left, device_id_type=MESH)

    loads = [
        pltpu.make_async_copy(a, b, load_sem.at[i])
        for i, (a, b) in enumerate(
            ((wc_hbm, wc), (wx_hbm, wx), (wb_hbm, wb), (wuk_hbm, wuk), (wuv_hbm, wuv),
             (wuq_hbm, wuq), (woa_hbm, woa), (woc_hbm, woc))
        )
    ]
    for load in loads:
        load.start()
    pl.semaphore_wait(barrier, 3 + jnp.where(has_right, 1, 0) + jnp.where(has_left, 1, 0))

    def remote(src, dst, send, recv, target):
        return pltpu.make_async_remote_copy(
            src_ref=src, dst_ref=dst, send_sem=send, recv_sem=recv,
            device_id=target, device_id_type=MESH,
        )

    def whole(kind, src, slot, lane, target):
        return remote(
            src, bufs[kind].at[slot], send_sem.at[kind, slot, lane], recv_sem.at[kind, slot], target
        )

    def half_of(kind, which):
        size = bufs[kind].shape[1] // 2
        return pl.ds(which * size, size)

    def half(kind, slot, which, target):
        place = bufs[kind].at[slot, half_of(kind, which)]
        return remote(
            place, place, send_sem.at[kind, slot, which], half_sem.at[kind, slot, which], target
        )

    def send_on(kinds, slot, left, right, own=False, along=True, across=True):
        for kind in kinds:
            src = owns[kind] if own else bufs[kind].at[slot]
            if along and right is not None:
                @pl.when(right)
                def _(kind=kind, src=src):
                    whole(kind, src, slot, 2, to_right).start()
            if along and left is not None:
                @pl.when(left)
                def _(kind=kind, src=src):
                    whole(kind, src, slot, 3, to_left).start()
            if across:
                whole(kind, src, slot, 0, to_x).start()
                whole(kind, src, slot, 1, to_y).start()

    def arrive(kinds, slot):
        for kind in kinds:
            whole(kind, bufs[kind].at[slot], slot, 0, to_x).wait_recv()

    def z_step(kinds, d):
        @pl.when(z - d >= 0)
        def _():
            slot = (z - d) * nf + f
            arrive(kinds, slot)
            send_on(kinds, slot, None, has_right)

        @pl.when(z + d < ns)
        def _():
            slot = (z + d) * nf + f
            arrive(kinds, slot)
            send_on(kinds, slot, has_left, None)

    def diag_at(kinds, zo):
        arrive(kinds, zo * nf + fx)
        for kind in kinds:
            half(kind, zo * nf + fx, 0, to_y).start()
        arrive(kinds, zo * nf + fy)
        for kind in kinds:
            half(kind, zo * nf + fy, 1, to_x).start()

    def diag_step(kinds, d):
        if d == 0:
            diag_at(kinds, z)
            return

        @pl.when(z - d >= 0)
        def _():
            diag_at(kinds, z - d)

        @pl.when(z + d < ns)
        def _():
            diag_at(kinds, z + d)

    def diag_done(kinds):
        for zo in range(ns):
            for kind in kinds:
                for which in range(2):
                    half(kind, zo * nf + fd, which, to_x).wait_recv()

    first, second = (KV, RK), (QL,)
    tok_copy = remote(tok, tok_in, tp_send.at[0], tp_recv.at[0], to_tp)
    tok_copy.start()
    send_on(first, me, has_left, has_right, own=True)
    send_on(second, me, None, None, own=True)
    wkv_buf[me] = kv_own[...]
    wr_buf[me] = wr[...]
    wq_buf[me] = q_own[...]

    def norm_rows(src, block):
        data = src[...].astype(F32)
        hid[pl.ds(pl.multiple_of(block * half_rows, half_rows), half_rows)] = normalize(
            data, h_gain[...]
        ).astype(BF16)

    norm_rows(tok, m)
    tok_copy.wait()
    norm_rows(tok_in, other)
    z_step(first, 1)
    send_on(second, me, has_left, has_right, own=True, across=False)

    width = 256
    tiles = wc.shape[1] // width
    pad = 8

    def conv_tile(t, carry):
        cols = pl.ds(pl.multiple_of(t * width, width), width)
        made = (dot(hid[...], wc[:, cols]) * dot(hid[...], wx[:, cols])).astype(BF16)
        cbuf[pl.ds(pad, rows), cols] = made.astype(F32)
        tail_out[:, cols] = made[rows - tail_out.shape[0] :]
        return carry

    loads[0].wait()
    loads[1].wait()
    diag_step(first, 0)
    conv_tile(0, 0)
    z_step(first, 2)
    diag_step(first, 1)
    lax.fori_loop(1, tiles, conv_tile, 0)
    tail_copy = remote(tail_out, tail_in, tail_sem.at[0], tail_sem.at[1], to_right)

    @pl.when(has_right)
    def _():
        tail_copy.start()

    z_step(second, 1)
    for d in range(3, ns):
        z_step(first, d)
        diag_step(first, d - 1)
    diag_step(second, 0)
    diag_step(first, ns - 1)
    angles = (
        z * rows + lax.broadcasted_iota(jnp.int32, cos_r.shape, 0)
    ).astype(F32) * inverse[...]
    lanes = lax.broadcasted_iota(jnp.int32, cos_r.shape, 1)
    cos_r[...] = jnp.cos(angles)
    sine = jnp.sin(angles)
    sin_r[...] = jnp.where(lanes < cos_r.shape[1] // 2, -sine, sine)
    z_step(second, 2)
    diag_step(second, 1)

    def rotated(data):
        return data * cos_r[...] + pltpu.roll(data, data.shape[1] // 2, 1) * sin_r[...]

    diag_done(first)
    depth = hid.shape[1]
    lat_kv[m] = dot(hid[...], wkv_buf[...].reshape(depth, kv_w))
    kv_copy = remote(lat_kv.at[m], lat_kv.at[m], tp_send.at[1], tp_recv.at[1], to_tp)
    kv_copy.start()
    w_rope = jnp.concatenate([wr_buf[s] for s in range(ns * nf)], axis=1)
    low, high = w_rope[: ROPE // 2], w_rope[ROPE // 2 :]
    rope = rotated(dot_t(hid[...], jnp.concatenate([low] * 4 + [high] * 4, axis=0)))
    rk_buf[0:rows] = rope.astype(BF16)
    flipped = rope.T
    rk[z] = jnp.concatenate(
        [flipped[: ROPE // 2], flipped[64 : 64 + ROPE // 2]], axis=0
    ).astype(BF16)
    for d in range(3, ns):
        z_step(second, d)
        diag_step(second, d - 1)

    def latent_norm(lat, gain):
        left, right = lat[0], lat[1]
        mean = (
            jnp.sum(left * left, axis=-1, keepdims=True)
            + jnp.sum(right * right, axis=-1, keepdims=True)
        ) / (2 * left.shape[1])
        scale = lax.rsqrt(mean + EPS)
        cut = left.shape[1]
        return (
            (left * scale * gain[:, :cut]).astype(BF16),
            (right * scale * gain[:, cut:]).astype(BF16),
        )

    kv_copy.wait()
    left, right = latent_norm(lat_kv, kv_gain[...])
    kvn[z, 0] = left
    kvn[z, 1] = right

    def kz(which, origin):
        ref = rk.at[origin]
        if which < 2:
            ref = kvn.at[origin, m, pl.ds(which * half_rows, half_rows)]
        return remote(ref, ref, kz_send.at[which, origin], kz_recv.at[which, origin], to_right)

    def kt(which, origin, part_of):
        ref = kvn.at[origin, part_of, pl.ds(which * half_rows, half_rows)]
        return remote(ref, ref, kt_send.at[which, origin], kt_recv.at[which, origin], to_tp)

    @pl.when(has_right)
    def _():
        for which in range(3):
            kz(which, z).start()

    @pl.when(has_left)
    def _():
        tail_copy.wait_recv()
        cbuf[0:pad] = tail_in[tail_in.shape[0] - pad :].astype(F32)

    @pl.when(jnp.logical_not(has_left))
    def _():
        cbuf[0:pad] = jnp.zeros((pad, cbuf.shape[1]), F32)

    loads[2].wait()

    def gate_tile(t, carry):
        cols = pl.ds(pl.multiple_of(t * width, width), width)
        gate = dot(hid[...], wb[:, cols])
        filtered = jnp.zeros((rows, width), F32)
        for tap in range(KW):
            start = pad - (KW - 1) + tap
            filtered = filtered + taps[tap : tap + 1, cols] * cbuf[pl.ds(start, rows), cols]
        conv_out[:, cols] = (gate * filtered).astype(BF16)
        return carry

    lax.fori_loop(0, tiles, gate_tile, 0)
    diag_step(second, ns - 1)
    loads[3].wait()
    loads[4].wait()

    def make_keys(d):
        origin = z - d
        lhs = jnp.concatenate([kvn[origin, 0], kvn[origin, 1]], axis=1)
        place = pl.ds(d * rows, rows)
        if d > 0:
            got = rk[origin].astype(F32)
            low, high = got[: ROPE // 2], got[ROPE // 2 :]
            rk_buf[place] = jnp.concatenate([low] * 4 + [high] * 4, axis=0).T.astype(BF16)

        def pair(p, carry):
            cols = pl.ds(pl.multiple_of(p * width, width), width)
            keys = dot(lhs, wuk[:, cols]).astype(BF16)
            vals = dot(lhs, wuv[:, cols]).astype(BF16)
            for i in range(2):
                k_buf[2 * p + i, place] = keys[:, 128 * i : 128 * (i + 1)]
                v_buf[2 * p + i, place] = vals[:, 128 * i : 128 * (i + 1)]
            return carry

        lax.fori_loop(0, wuk.shape[1] // width, pair, 0)

    def take_keys(d):
        @pl.when(z - d >= 0)
        def _():
            origin = z - d
            for which in (0, 1, 2):
                kz(which, origin).wait_recv()

                @pl.when(has_right)
                def _(which=which):
                    kz(which, origin).start()

                if which < 2:
                    kt(which, origin, m).start()

    def use_keys(d):
        @pl.when(z - d >= 0)
        def _():
            kt(0, z - d, other).wait_recv()
            kt(1, z - d, other).wait_recv()
            make_keys(d)

    make_keys(0)
    head = NOPE + ROPE
    heads = wuq.shape[1] // head
    loads[5].wait()
    take_keys(1)
    for p in range(heads // 2):
        wn[:, 128 * p : 128 * (p + 1)] = jnp.concatenate(
            [wuq[:, h * head : h * head + NOPE] for h in (2 * p, 2 * p + 1)], axis=1
        )
    for g in range(heads // 4):
        wp[:, 128 * g : 128 * (g + 1)] = jnp.concatenate(
            [
                wuq[:, h * head + NOPE + 16 * i : h * head + NOPE + 16 * (i + 1)]
                for i in range(2) for h in range(4 * g, 4 * g + 4)
            ],
            axis=1,
        )
    for d in range(2, ns):
        take_keys(d)
        use_keys(d - 1)
    diag_done(second)
    lat_q[m] = dot(hid[...], wq_buf[...].reshape(depth, q_w))
    q_copy = remote(lat_q.at[m], lat_q.at[m], tp_send.at[2], tp_recv.at[2], to_tp)
    q_copy.start()
    use_keys(ns - 1)
    q_copy.wait()
    gains = q_gain[...].reshape(1, -1)
    q_left, q_right = latent_norm(lat_q, gains)
    q_norm = jnp.concatenate([q_left, q_right], axis=1)
    nope = dot(q_norm, wn[...])
    roped = dot(q_norm, wp[...])
    for p in range(heads // 2):
        q_buf[p] = nope[:, 128 * p : 128 * (p + 1)].astype(BF16)
    for g in range(heads // 4):
        q_rope[g] = rotated(roped[:, 128 * g : 128 * (g + 1)]).astype(BF16)

    lane = lax.broadcasted_iota(jnp.int32, (rows, 128), 1)
    factor = head ** (-0.5) * 1.4426950408889634

    def attend(blocks):
        span = blocks * rows
        seen = lax.broadcasted_iota(jnp.int32, (rows, rows), 1) <= (
            lax.broadcasted_iota(jnp.int32, (rows, rows), 0)
        )

        def pair(p, carry):
            keys = jnp.concatenate([k_buf[p, 0:span], rk_buf[0:span]], axis=1)
            vals = v_buf[p, 0:span]
            nope = q_buf[p].astype(F32)
            roped = q_rope[p // 2].astype(F32)
            done = []
            for i in range(2):
                mine = jnp.where(lane // NOPE == i, nope, 0.0)
                turn = jnp.where((lane // 16) % 4 == (2 * p + i) % 4, roped, 0.0)
                scores = dot_t(jnp.concatenate([mine, turn], axis=1).astype(BF16), keys)
                near = jnp.where(seen, scores[:, :rows], -jnp.inf)
                if blocks > 1:
                    scores = jnp.concatenate([near, scores[:, rows:]], axis=1)
                else:
                    scores = near
                largest = jnp.max(scores, axis=-1, keepdims=True)
                weights = jnp.exp2((scores - largest) * factor)
                total = jnp.sum(weights, axis=-1, keepdims=True)
                done.append(dot(weights.astype(BF16), vals) / total)
            a_buf[p] = jnp.where(lane < VH, done[0], done[1]).astype(BF16)
            return carry

        lax.fori_loop(0, heads // 2, pair, 0)

    for d in range(ns):
        @pl.when(z == d)
        def _(d=d):
            attend(d + 1)

    attn = jnp.concatenate([a_buf[p] for p in range(heads // 2)], axis=1)
    loads[6].wait()
    loads[7].wait()
    step = 512

    def out_copy(t):
        cols = pl.ds(pl.multiple_of(t * step, step), step)
        return remote(
            part.at[other, :, cols], part_in.at[:, cols], out_send.at[t], out_recv.at[t], to_tp
        )

    def project(t, carry):
        cols = pl.ds(pl.multiple_of(t * step, step), step)
        term = (dot(attn, woa[:, cols]) + dot(conv_out[...], woc[:, cols])).astype(BF16)
        part[0, :, cols] = term[:half_rows]
        part[1, :, cols] = term[half_rows:]
        out_copy(t).start()
        return carry

    count = out.shape[1] // step
    lax.fori_loop(0, count, project, 0)

    def finish(t, carry):
        cols = pl.ds(pl.multiple_of(t * step, step), step)
        out_copy(t).wait_recv()
        out[:, cols] = (part[m, :, cols].astype(F32) + part_in[:, cols].astype(F32)).astype(BF16)
        return carry

    lax.fori_loop(0, count, finish, 0)

    def sent_slot(kind, slot, left, right):
        ref = bufs[kind].at[slot]
        if right is not None:
            @pl.when(right)
            def _():
                whole(kind, ref, slot, 2, to_right).wait_send()
        if left is not None:
            @pl.when(left)
            def _():
                whole(kind, ref, slot, 3, to_left).wait_send()
        whole(kind, ref, slot, 0, to_x).wait_send()
        whole(kind, ref, slot, 1, to_y).wait_send()

    for kind in (KV, RK, QL):
        sent_slot(kind, me, has_left, has_right)
        for d in range(1, ns):
            @pl.when(z - d >= 0)
            def _(d=d, kind=kind):
                sent_slot(kind, (z - d) * nf + f, None, has_right)

            @pl.when(z + d < ns)
            def _(d=d, kind=kind):
                sent_slot(kind, (z + d) * nf + f, has_left, None)
        for zo in range(ns):
            half(kind, zo * nf + fx, 0, to_y).wait_send()
            half(kind, zo * nf + fy, 1, to_x).wait_send()

    @pl.when(has_right)
    def _():
        tail_copy.wait_send()
        for d in range(ns):
            @pl.when(z - d >= 0)
            def _(d=d):
                for which in range(3):
                    kz(which, z - d).wait_send()

    for d in range(1, ns):
        @pl.when(z - d >= 0)
        def _(d=d):
            kt(0, z - d, m).wait_send()
            kt(1, z - d, m).wait_send()

    def sent_out(t, carry):
        out_copy(t).wait_send()
        return carry

    lax.fori_loop(0, count, sent_out, 0)


def fused_device(
    ns, nf, tokens, h_gain, w_qlat, w_kvlat, w_krope, q_gain, kv_gain, w_uq, w_uk, w_uv,
    w_convb, w_convc, w_convx, conv_taps, w_out_attn, w_out_conv,
):
    half_rows, depth = tokens.shape[1:]
    rows = 2 * half_rows
    slots = ns * nf
    cut = w_qlat.shape[0]
    heads = w_uk.shape[1] // NOPE
    inverse = jnp.tile(THETA ** (-jnp.arange(0, ROPE, 2, dtype=F32) / ROPE), 8)[None]
    vmem = pl.BlockSpec(memory_space=pltpu.VMEM)
    anywhere = pl.BlockSpec(memory_space=pl.ANY)
    V, DMA = pltpu.VMEM, pltpu.SemaphoreType.DMA
    big = (w_convb, w_convc, w_convx, w_uq, w_uk, w_uv, w_out_attn, w_out_conv)
    span = ns * rows
    q_w, kv_w = w_qlat.shape[1] // 2, w_kvlat.shape[1] // 2
    result = pl.pallas_call(
        functools.partial(fused_kernel, ns, nf),
        out_shape=jax.ShapeDtypeStruct((half_rows, depth), BF16),
        in_specs=[vmem] * 9 + [anywhere] * 8,
        out_specs=vmem,
        scratch_shapes=[
            V((half_rows, depth), BF16), V((rows, depth), BF16),
            V((slots, cut, q_w), BF16), V((slots, cut, kv_w), BF16), V((slots, ROPE, cut), BF16),
        ] + [V(w.shape, BF16) for w in big] + [
            V((rows + 8, w_convc.shape[1]), F32),
            V((16, w_convc.shape[1]), BF16), V((16, w_convc.shape[1]), BF16),
            V((rows, w_convc.shape[1]), BF16),
            V((2, rows, kv_w), F32), V((2, rows, q_w), F32),
            V((ns, 2, rows, kv_w), BF16), V((ns, ROPE, rows), BF16),
            V((heads // 2, span, 2 * NOPE), BF16), V((span, 128), BF16),
            V((heads // 2, span, 2 * VH), BF16),
            V((w_uq.shape[0], heads * NOPE), BF16), V((w_uq.shape[0], heads * ROPE), BF16),
            V((rows, 128), F32), V((rows, 128), F32),
            V((heads // 4, rows, 128), BF16), V((heads // 2, rows, 2 * NOPE), BF16),
            V((heads // 2, rows, 2 * VH), BF16),
            V((2, half_rows, depth), BF16), V((half_rows, depth), BF16),
            DMA((8,)), DMA((3, slots, 4)), DMA((3, slots)), DMA((3, slots, 2)),
            DMA((3,)), DMA((3,)), DMA((3, ns)), DMA((3, ns)), DMA((2, ns)), DMA((2, ns)),
            DMA((2,)), DMA((4,)), DMA((4,)),
        ],
        compiler_params=pltpu.CompilerParams(
            collective_id=0, has_side_effects=True, vmem_limit_bytes=60 * 1024 * 1024
        ),
    )(
        tokens[0], h_gain[None], w_qlat, w_kvlat, w_krope.T, q_gain, kv_gain[None],
        conv_taps, inverse, *big,
    )
    return result[None]


def solution(mesh):
    in_specs = (
        P("fs", ("sp", "tp"), None),
        P(),
        P(("sp", "fs"), None),
        P(("sp", "fs"), None),
        P(("sp", "fs"), None),
        P(),
        P(),
        P(None, "tp"),
        P(None, "tp"),
        P(None, "tp"),
        P(None, "tp"),
        P(None, "tp"),
        P(None, "tp"),
        P(None, "tp"),
        P("tp", None),
        P("tp", None),
    )
    out_specs = P("fs", ("sp", "tp"), None)
    fits = mesh.shape["tp"] == 2 and mesh.shape["fs"] == 4
    body = functools.partial(fused_device, mesh.shape["sp"], mesh.shape["fs"]) if fits else per_device
    return jax.shard_map(
        body, mesh=mesh, in_specs=in_specs, out_specs=out_specs, check_vma=False
    )
```

```python
import functools

import jax
import jax.numpy as jnp
from jax import lax
from jax.experimental import pallas as pl
from jax.experimental.pallas import tpu as pltpu
from jax.sharding import PartitionSpec as P

NOPE = 64
ROPE = 32
VH = 64
KW = 3


EPS = 1e-06
THETA = 10000.0
NEG_START = -1e30


def from_behind(array, axis, by):
    size = lax.axis_size(axis)
    pairs = [(i, i + by) for i in range(size) if 0 <= i + by < size]
    return lax.ppermute(array, axis, pairs)


def normalize(values_in, gain):
    return (
        values_in * lax.rsqrt(jnp.mean(values_in * values_in, axis=-1, keepdims=True) + EPS) * gain
    )


def angle_table(positions, dims):
    inverse = THETA ** (-jnp.arange(0, dims, 2, dtype=jnp.float32) / dims)
    return positions[:, None] * inverse


def rotate(values_in, angles):
    lower_half, upper_half = jnp.split(values_in, 2, axis=-1)
    cosine = jnp.cos(angles)
    sine_part = jnp.sin(angles)
    return jnp.concatenate(
        [
            lower_half * cosine - upper_half * sine_part,
            lower_half * sine_part + upper_half * cosine,
        ],
        axis=-1,
    )


def per_device(
    tokens,
    h_gain,
    w_qlat,
    w_kvlat,
    w_krope,
    q_gain,
    kv_gain,
    w_uq,
    w_uk,
    w_uv,
    w_convb,
    w_convc,
    w_convx,
    conv_taps,
    w_out_attn,
    w_out_conv,
):
    own_rows = lax.all_gather(tokens, "tp", axis=1, tiled=True)
    seq_count = own_rows.shape[0]
    rows_here = own_rows.shape[1]
    flat_count = seq_count * rows_here
    hidden = normalize(own_rows.astype(jnp.float32), h_gain).astype(jnp.bfloat16)
    flat_hidden = hidden.reshape(flat_count, hidden.shape[2])
    groups = lax.axis_size("tp")
    member = lax.axis_index("tp")
    q_cols = w_qlat.shape[1] // groups
    kv_cols = w_kvlat.shape[1] // groups
    rope_cols = w_krope.shape[1] // groups
    q_part = lax.dynamic_slice_in_dim(w_qlat, member * q_cols, q_cols, 1)
    kv_part = lax.dynamic_slice_in_dim(w_kvlat, member * kv_cols, kv_cols, 1)
    rope_part = lax.dynamic_slice_in_dim(w_krope, member * rope_cols, rope_cols, 1)
    whole_q, whole_kv, whole_rope = (
        lax.all_gather(q_part, ("sp", "fs"), axis=0, tiled=True),
        lax.all_gather(kv_part, ("sp", "fs"), axis=0, tiled=True),
        lax.all_gather(rope_part, ("sp", "fs"), axis=0, tiled=True),
    )
    partial_latents = (
        jnp.dot(flat_hidden, whole_q, preferred_element_type=jnp.float32),
        jnp.dot(flat_hidden, whole_kv, preferred_element_type=jnp.float32),
        jnp.dot(flat_hidden, whole_rope, preferred_element_type=jnp.float32),
    )
    query_latent, kv_latent, rope_latent = (
        lax.all_gather(partial_latents[0], "tp", axis=1, tiled=True),
        lax.all_gather(partial_latents[1], "tp", axis=1, tiled=True),
        lax.all_gather(partial_latents[2], "tp", axis=1, tiled=True),
    )
    query_latent = query_latent.reshape(seq_count, rows_here, query_latent.shape[1])
    kv_latent = kv_latent.reshape(seq_count, rows_here, kv_latent.shape[1])
    rope_latent = rope_latent.reshape(seq_count, rows_here, rope_latent.shape[1])
    base = lax.axis_index("sp") * rows_here
    query_pos = base + jnp.arange(rows_here, dtype=jnp.int32)
    angles = angle_table(query_pos.astype(jnp.float32), ROPE)
    query_norm = normalize(query_latent, q_gain).astype(jnp.bfloat16)
    kv_norm = normalize(kv_latent, kv_gain).astype(jnp.bfloat16)
    rope_key = rotate(rope_latent, angles[None]).astype(jnp.bfloat16)
    head_count = w_uk.shape[1] // NOPE
    query = jnp.einsum("sqc,cn->sqn", query_norm, w_uq, preferred_element_type=jnp.float32).reshape(
        seq_count, rows_here, head_count, NOPE + ROPE
    )
    query = jnp.concatenate(
        [query[..., :NOPE], rotate(query[..., NOPE:], angles[None, :, None, :])], axis=-1
    ).astype(jnp.bfloat16)
    query = query.transpose(0, 2, 1, 3)
    score_scale = (NOPE + ROPE) ** (-0.5)
    last_query = base + rows_here - 1
    fold_start = (
        jnp.full((seq_count, head_count, rows_here), NEG_START, jnp.float32),
        jnp.zeros((seq_count, head_count, rows_here), jnp.float32),
        jnp.zeros((seq_count, head_count, rows_here, VH), jnp.float32),
    )
    pieces = (
        lax.all_gather(kv_norm, "sp", axis=1, tiled=True),
        lax.all_gather(rope_key, "sp", axis=1, tiled=True),
    )

    def make_keys():
        key_nope = jnp.einsum(
            "skc,cn->skn", pieces[0], w_uk, preferred_element_type=jnp.float32
        ).astype(jnp.bfloat16)
        value_rows = jnp.einsum(
            "skc,cn->skn", pieces[0], w_uv, preferred_element_type=jnp.float32
        ).astype(jnp.bfloat16)
        return (key_nope, value_rows, pieces[1])

    def compute(state):
        running_max, running_sum, weighted = state
        key_nope, value_rows, rope_piece = make_keys()
        width = rope_piece.shape[1]
        keys = jnp.concatenate(
            [
                key_nope.reshape(seq_count, width, head_count, NOPE),
                jnp.broadcast_to(rope_piece[:, :, None, :], (seq_count, width, head_count, ROPE)),
            ],
            axis=-1,
        )
        scores = (
            jnp.einsum("shqd,skhd->shqk", query, keys, preferred_element_type=jnp.float32)
            * score_scale
        )
        key_pos = jnp.arange(width, dtype=jnp.int32)
        visible = key_pos[None, :] <= query_pos[:, None]
        scores = jnp.where(visible[None, None], scores, -jnp.inf)
        new_max = jnp.maximum(running_max, jnp.max(scores, axis=-1))
        weights = jnp.exp(scores - new_max[..., None])
        new_sum = jnp.sum(weights, axis=-1)
        update = jnp.einsum(
            "shqk,skhv->shqv",
            weights.astype(jnp.bfloat16),
            value_rows.reshape(seq_count, width, head_count, VH),
            preferred_element_type=jnp.float32,
        )
        return (new_max, new_sum, update)

    def keep(state):
        return state

    final = lax.cond(jnp.int32(0) <= last_query, compute, keep, fold_start)
    attn = (
        (final[2] / final[1][..., None])
        .transpose(0, 2, 1, 3)
        .reshape(seq_count, rows_here, head_count * VH)
        .astype(jnp.bfloat16)
    )
    conv_b = jnp.dot(flat_hidden, w_convb, preferred_element_type=jnp.float32).reshape(
        seq_count, rows_here, w_convb.shape[1]
    )
    conv_c = jnp.dot(flat_hidden, w_convc, preferred_element_type=jnp.float32)
    conv_x = jnp.dot(flat_hidden, w_convx, preferred_element_type=jnp.float32)
    conv_in = (conv_c * conv_x).astype(jnp.bfloat16).reshape(seq_count, rows_here, w_convc.shape[1])
    edge_rows = from_behind(conv_in[:, rows_here - (KW - 1) :], "sp", 1)
    padded = jnp.concatenate([edge_rows, conv_in], axis=1).astype(jnp.float32)
    filtered = jnp.zeros(conv_b.shape, jnp.float32)
    for tap in range(KW):
        filtered = filtered + conv_taps[tap] * padded[:, tap : tap + rows_here]
    conv_out = (conv_b * filtered).astype(jnp.bfloat16)
    result = lax.psum_scatter(
        (
            jnp.einsum("sqc,cd->qsd", attn, w_out_attn, preferred_element_type=jnp.float32)
            + jnp.einsum("sqc,cd->qsd", conv_out, w_out_conv, preferred_element_type=jnp.float32)
        ).astype(jnp.bfloat16),
        "tp",
        scatter_dimension=0,
        tiled=True,
    )
    return result.transpose(1, 0, 2)


MESH = pl.DeviceIdType.MESH
F32 = jnp.float32
BF16 = jnp.bfloat16
KV, RK, QL = 0, 1, 2


def dot(a, b):
    return jnp.dot(a, b, preferred_element_type=F32)


def dot_t(a, b):
    return lax.dot_general(a, b, (((1,), (1,)), ((), ())), preferred_element_type=F32)


def fused_kernel(
    ns, nf,
    tok, h_gain, wq, wkv, wr, q_gain, kv_gain, taps, inverse,
    wb_hbm, wc_hbm, wx_hbm, wuq_hbm, wuk_hbm, wuv_hbm, woa_hbm, woc_hbm,
    out,
    tok_in, hid, wq_buf, wkv_buf, wr_buf, wb, wc, wx, wuq, wuk, wuv, woa, woc,
    cbuf, tail_out, tail_in, conv_out,
    lat_kv, lat_q, kvn, rk, k_buf, rk_buf, v_buf, wn, wp, cos_r, sin_r, q_rope, q_buf, a_buf, part, part_in,
    load_sem, send_sem, recv_sem, half_sem, tp_send, tp_recv, kz_send, kz_recv, kt_send, kt_recv,
    tail_sem, out_send, out_recv,
):
    z, f, m = lax.axis_index("sp"), lax.axis_index("fs"), lax.axis_index("tp")
    fx = f + 1 - 2 * (f % 2)
    fy = (f + 2) % 4
    fd = fx + 2 - 4 * (fx // 2)
    other = 1 - m
    to_x, to_y, to_tp = {"fs": fx}, {"fs": fy}, {"tp": other}
    to_right, to_left = {"sp": z + 1}, {"sp": z - 1}
    half_rows, rows = tok.shape[0], hid.shape[0]
    has_right, has_left = z < ns - 1, z > 0
    bufs = (wkv_buf, wr_buf, wq_buf)
    kv_w, q_w = wkv_buf.shape[2], wq_buf.shape[2]
    kv_own = wkv.at[:, pl.ds(pl.multiple_of(m * kv_w, kv_w), kv_w)]
    q_own = wq.at[:, pl.ds(pl.multiple_of(m * q_w, q_w), q_w)]
    owns = (kv_own, wr, q_own)
    me = z * nf + f

    barrier = pltpu.get_barrier_semaphore()
    for target in (to_x, to_y, to_tp):
        pl.semaphore_signal(barrier, inc=1, device_id=target, device_id_type=MESH)

    @pl.when(has_right)
    def _():
        pl.semaphore_signal(barrier, inc=1, device_id=to_right, device_id_type=MESH)

    @pl.when(has_left)
    def _():
        pl.semaphore_signal(barrier, inc=1, device_id=to_left, device_id_type=MESH)

    loads = [
        pltpu.make_async_copy(a, b, load_sem.at[i])
        for i, (a, b) in enumerate(
            ((wc_hbm, wc), (wx_hbm, wx), (wb_hbm, wb), (wuk_hbm, wuk), (wuv_hbm, wuv),
             (wuq_hbm, wuq), (woa_hbm, woa), (woc_hbm, woc))
        )
    ]
    for load in loads:
        load.start()
    pl.semaphore_wait(barrier, 3 + jnp.where(has_right, 1, 0) + jnp.where(has_left, 1, 0))

    def remote(src, dst, send, recv, target):
        return pltpu.make_async_remote_copy(
            src_ref=src, dst_ref=dst, send_sem=send, recv_sem=recv,
            device_id=target, device_id_type=MESH,
        )

    def whole(kind, src, slot, lane, target):
        return remote(
            src, bufs[kind].at[slot], send_sem.at[kind, slot, lane], recv_sem.at[kind, slot], target
        )

    def half_of(kind, which):
        size = bufs[kind].shape[1] // 2
        return pl.ds(which * size, size)

    def half(kind, slot, which, target):
        place = bufs[kind].at[slot, half_of(kind, which)]
        return remote(
            place, place, send_sem.at[kind, slot, which], half_sem.at[kind, slot, which], target
        )

    def send_on(kinds, slot, left, right, own=False, along=True, across=True):
        for kind in kinds:
            src = owns[kind] if own else bufs[kind].at[slot]
            if along and right is not None:
                @pl.when(right)
                def _(kind=kind, src=src):
                    whole(kind, src, slot, 2, to_right).start()
            if along and left is not None:
                @pl.when(left)
                def _(kind=kind, src=src):
                    whole(kind, src, slot, 3, to_left).start()
            if across:
                whole(kind, src, slot, 0, to_x).start()
                whole(kind, src, slot, 1, to_y).start()

    def arrive(kinds, slot):
        for kind in kinds:
            whole(kind, bufs[kind].at[slot], slot, 0, to_x).wait_recv()

    def z_step(kinds, d):
        @pl.when(z - d >= 0)
        def _():
            slot = (z - d) * nf + f
            arrive(kinds, slot)
            send_on(kinds, slot, None, has_right)

        @pl.when(z + d < ns)
        def _():
            slot = (z + d) * nf + f
            arrive(kinds, slot)
            send_on(kinds, slot, has_left, None)

    def diag_at(kinds, zo):
        arrive(kinds, zo * nf + fx)
        for kind in kinds:
            half(kind, zo * nf + fx, 0, to_y).start()
        arrive(kinds, zo * nf + fy)
        for kind in kinds:
            half(kind, zo * nf + fy, 1, to_x).start()

    def diag_step(kinds, d):
        if d == 0:
            diag_at(kinds, z)
            return

        @pl.when(z - d >= 0)
        def _():
            diag_at(kinds, z - d)

        @pl.when(z + d < ns)
        def _():
            diag_at(kinds, z + d)

    def diag_done(kinds):
        for zo in range(ns):
            for kind in kinds:
                for which in range(2):
                    half(kind, zo * nf + fd, which, to_x).wait_recv()

    first, second = (KV, RK), (QL,)
    tok_copy = remote(tok, tok_in, tp_send.at[0], tp_recv.at[0], to_tp)
    tok_copy.start()
    send_on(first, me, has_left, has_right, own=True)
    send_on(second, me, None, None, own=True)
    wkv_buf[me] = kv_own[...]
    wr_buf[me] = wr[...]
    wq_buf[me] = q_own[...]

    def norm_rows(src, block):
        data = src[...].astype(F32)
        hid[pl.ds(pl.multiple_of(block * half_rows, half_rows), half_rows)] = normalize(
            data, h_gain[...]
        ).astype(BF16)

    norm_rows(tok, m)
    tok_copy.wait()
    norm_rows(tok_in, other)
    z_step(first, 1)
    send_on(second, me, has_left, has_right, own=True, across=False)

    width = 256
    tiles = wc.shape[1] // width
    pad = 8

    def conv_tile(t, carry):
        cols = pl.ds(pl.multiple_of(t * width, width), width)
        made = (dot(hid[...], wc[:, cols]) * dot(hid[...], wx[:, cols])).astype(BF16)
        cbuf[pl.ds(pad, rows), cols] = made.astype(F32)
        tail_out[:, cols] = made[rows - tail_out.shape[0] :]
        return carry

    loads[0].wait()
    loads[1].wait()
    diag_step(first, 0)
    conv_tile(0, 0)
    z_step(first, 2)
    diag_step(first, 1)
    lax.fori_loop(1, tiles, conv_tile, 0)
    tail_copy = remote(tail_out, tail_in, tail_sem.at[0], tail_sem.at[1], to_right)

    @pl.when(has_right)
    def _():
        tail_copy.start()

    z_step(second, 1)
    for d in range(3, ns):
        z_step(first, d)
        diag_step(first, d - 1)
    diag_step(second, 0)
    diag_step(first, ns - 1)
    angles = (
        z * rows + lax.broadcasted_iota(jnp.int32, cos_r.shape, 0)
    ).astype(F32) * inverse[...]
    lanes = lax.broadcasted_iota(jnp.int32, cos_r.shape, 1)
    cos_r[...] = jnp.cos(angles)
    sine = jnp.sin(angles)
    sin_r[...] = jnp.where(lanes < cos_r.shape[1] // 2, -sine, sine)
    z_step(second, 2)
    diag_step(second, 1)

    def rotated(data):
        return data * cos_r[...] + pltpu.roll(data, data.shape[1] // 2, 1) * sin_r[...]

    diag_done(first)
    depth = hid.shape[1]
    lat_kv[m] = dot(hid[...], wkv_buf[...].reshape(depth, kv_w))
    kv_copy = remote(lat_kv.at[m], lat_kv.at[m], tp_send.at[1], tp_recv.at[1], to_tp)
    kv_copy.start()
    w_rope = jnp.concatenate([wr_buf[s] for s in range(ns * nf)], axis=1)
    low, high = w_rope[: ROPE // 2], w_rope[ROPE // 2 :]
    rope = rotated(dot_t(hid[...], jnp.concatenate([low] * 4 + [high] * 4, axis=0)))
    rk_buf[0:rows] = rope.astype(BF16)
    flipped = rope.T
    rk[z] = jnp.concatenate(
        [flipped[: ROPE // 2], flipped[64 : 64 + ROPE // 2]], axis=0
    ).astype(BF16)
    for d in range(3, ns):
        z_step(second, d)
        diag_step(second, d - 1)

    def latent_norm(lat, gain):
        left, right = lat[0], lat[1]
        mean = (
            jnp.sum(left * left, axis=-1, keepdims=True)
            + jnp.sum(right * right, axis=-1, keepdims=True)
        ) / (2 * left.shape[1])
        scale = lax.rsqrt(mean + EPS)
        cut = left.shape[1]
        return (
            (left * scale * gain[:, :cut]).astype(BF16),
            (right * scale * gain[:, cut:]).astype(BF16),
        )

    kv_copy.wait()
    left, right = latent_norm(lat_kv, kv_gain[...])
    kvn[z, 0] = left
    kvn[z, 1] = right

    def kz(which, origin):
        ref = rk.at[origin]
        if which < 2:
            ref = kvn.at[origin, m, pl.ds(which * half_rows, half_rows)]
        return remote(ref, ref, kz_send.at[which, origin], kz_recv.at[which, origin], to_right)

    def kt(which, origin, part_of):
        ref = kvn.at[origin, part_of, pl.ds(which * half_rows, half_rows)]
        return remote(ref, ref, kt_send.at[which, origin], kt_recv.at[which, origin], to_tp)

    @pl.when(has_right)
    def _():
        for which in range(3):
            kz(which, z).start()

    @pl.when(has_left)
    def _():
        tail_copy.wait_recv()
        cbuf[0:pad] = tail_in[tail_in.shape[0] - pad :].astype(F32)

    @pl.when(jnp.logical_not(has_left))
    def _():
        cbuf[0:pad] = jnp.zeros((pad, cbuf.shape[1]), F32)

    loads[2].wait()

    def gate_tile(t, carry):
        cols = pl.ds(pl.multiple_of(t * width, width), width)
        gate = dot(hid[...], wb[:, cols])
        filtered = jnp.zeros((rows, width), F32)
        for tap in range(KW):
            start = pad - (KW - 1) + tap
            filtered = filtered + taps[tap : tap + 1, cols] * cbuf[pl.ds(start, rows), cols]
        conv_out[:, cols] = (gate * filtered).astype(BF16)
        return carry

    lax.fori_loop(0, tiles, gate_tile, 0)
    diag_step(second, ns - 1)
    loads[3].wait()
    loads[4].wait()

    def make_keys(d):
        origin = z - d
        lhs = jnp.concatenate([kvn[origin, 0], kvn[origin, 1]], axis=1)
        place = pl.ds(d * rows, rows)
        if d > 0:
            got = rk[origin].astype(F32)
            low, high = got[: ROPE // 2], got[ROPE // 2 :]
            rk_buf[place] = jnp.concatenate([low] * 4 + [high] * 4, axis=0).T.astype(BF16)

        def pair(p, carry):
            cols = pl.ds(pl.multiple_of(p * width, width), width)
            keys = dot(lhs, wuk[:, cols]).astype(BF16)
            vals = dot(lhs, wuv[:, cols]).astype(BF16)
            for i in range(2):
                k_buf[2 * p + i, place] = keys[:, 128 * i : 128 * (i + 1)]
                v_buf[2 * p + i, place] = vals[:, 128 * i : 128 * (i + 1)]
            return carry

        lax.fori_loop(0, wuk.shape[1] // width, pair, 0)

    def take_keys(d):
        @pl.when(z - d >= 0)
        def _():
            origin = z - d
            for which in (0, 1, 2):
                kz(which, origin).wait_recv()

                @pl.when(has_right)
                def _(which=which):
                    kz(which, origin).start()

                if which < 2:
                    kt(which, origin, m).start()

    def use_keys(d):
        @pl.when(z - d >= 0)
        def _():
            kt(0, z - d, other).wait_recv()
            kt(1, z - d, other).wait_recv()
            make_keys(d)

    make_keys(0)
    head = NOPE + ROPE
    heads = wuq.shape[1] // head
    loads[5].wait()
    take_keys(1)
    for p in range(heads // 2):
        wn[:, 128 * p : 128 * (p + 1)] = jnp.concatenate(
            [wuq[:, h * head : h * head + NOPE] for h in (2 * p, 2 * p + 1)], axis=1
        )
    for g in range(heads // 4):
        wp[:, 128 * g : 128 * (g + 1)] = jnp.concatenate(
            [
                wuq[:, h * head + NOPE + 16 * i : h * head + NOPE + 16 * (i + 1)]
                for i in range(2) for h in range(4 * g, 4 * g + 4)
            ],
            axis=1,
        )
    for d in range(2, ns - 1):
        take_keys(d)
        use_keys(d - 1)
    diag_done(second)
    lat_q[m] = dot(hid[...], wq_buf[...].reshape(depth, q_w))
    q_copy = remote(lat_q.at[m], lat_q.at[m], tp_send.at[2], tp_recv.at[2], to_tp)
    q_copy.start()
    if ns > 2:
        use_keys(ns - 2)
    q_copy.wait()
    gains = q_gain[...].reshape(1, -1)
    q_left, q_right = latent_norm(lat_q, gains)
    q_norm = jnp.concatenate([q_left, q_right], axis=1)
    nope = dot(q_norm, wn[...])
    roped = dot(q_norm, wp[...])
    for p in range(heads // 2):
        q_buf[p] = nope[:, 128 * p : 128 * (p + 1)].astype(BF16)
    for g in range(heads // 4):
        q_rope[g] = rotated(roped[:, 128 * g : 128 * (g + 1)]).astype(BF16)
    if ns > 2:
        take_keys(ns - 1)
    use_keys(ns - 1)

    lane = lax.broadcasted_iota(jnp.int32, (rows, 128), 1)
    factor = head ** (-0.5) * 1.4426950408889634

    def attend(blocks):
        span = blocks * rows
        seen = lax.broadcasted_iota(jnp.int32, (rows, rows), 1) <= (
            lax.broadcasted_iota(jnp.int32, (rows, rows), 0)
        )

        def pair(p, carry):
            keys = jnp.concatenate([k_buf[p, 0:span], rk_buf[0:span]], axis=1)
            vals = v_buf[p, 0:span]
            nope = q_buf[p].astype(F32)
            roped = q_rope[p // 2].astype(F32)
            done = []
            for i in range(2):
                mine = jnp.where(lane // NOPE == i, nope, 0.0)
                turn = jnp.where((lane // 16) % 4 == (2 * p + i) % 4, roped, 0.0)
                scores = dot_t(jnp.concatenate([mine, turn], axis=1).astype(BF16), keys)
                near = jnp.where(seen, scores[:, :rows], -jnp.inf)
                if blocks > 1:
                    scores = jnp.concatenate([near, scores[:, rows:]], axis=1)
                else:
                    scores = near
                largest = jnp.max(scores, axis=-1, keepdims=True)
                weights = jnp.exp2((scores - largest) * factor)
                total = jnp.sum(weights, axis=-1, keepdims=True)
                done.append(dot(weights.astype(BF16), vals) / total)
            a_buf[p] = jnp.where(lane < VH, done[0], done[1]).astype(BF16)
            return carry

        lax.fori_loop(0, heads // 2, pair, 0)

    for d in range(ns):
        @pl.when(z == d)
        def _(d=d):
            attend(d + 1)

    attn = jnp.concatenate([a_buf[p] for p in range(heads // 2)], axis=1)
    loads[6].wait()
    loads[7].wait()
    step = 512

    def out_copy(t):
        cols = pl.ds(pl.multiple_of(t * step, step), step)
        return remote(
            part.at[other, :, cols], part_in.at[:, cols], out_send.at[t], out_recv.at[t], to_tp
        )

    def project(t, carry):
        cols = pl.ds(pl.multiple_of(t * step, step), step)
        term = (dot(attn, woa[:, cols]) + dot(conv_out[...], woc[:, cols])).astype(BF16)
        part[0, :, cols] = term[:half_rows]
        part[1, :, cols] = term[half_rows:]
        out_copy(t).start()
        return carry

    count = out.shape[1] // step
    lax.fori_loop(0, count, project, 0)

    def finish(t, carry):
        cols = pl.ds(pl.multiple_of(t * step, step), step)
        out_copy(t).wait_recv()
        out[:, cols] = (part[m, :, cols].astype(F32) + part_in[:, cols].astype(F32)).astype(BF16)
        return carry

    lax.fori_loop(0, count, finish, 0)

    def sent_slot(kind, slot, left, right):
        ref = bufs[kind].at[slot]
        if right is not None:
            @pl.when(right)
            def _():
                whole(kind, ref, slot, 2, to_right).wait_send()
        if left is not None:
            @pl.when(left)
            def _():
                whole(kind, ref, slot, 3, to_left).wait_send()
        whole(kind, ref, slot, 0, to_x).wait_send()
        whole(kind, ref, slot, 1, to_y).wait_send()

    for kind in (KV, RK, QL):
        sent_slot(kind, me, has_left, has_right)
        for d in range(1, ns):
            @pl.when(z - d >= 0)
            def _(d=d, kind=kind):
                sent_slot(kind, (z - d) * nf + f, None, has_right)

            @pl.when(z + d < ns)
            def _(d=d, kind=kind):
                sent_slot(kind, (z + d) * nf + f, has_left, None)
        for zo in range(ns):
            half(kind, zo * nf + fx, 0, to_y).wait_send()
            half(kind, zo * nf + fy, 1, to_x).wait_send()

    @pl.when(has_right)
    def _():
        tail_copy.wait_send()
        for d in range(ns):
            @pl.when(z - d >= 0)
            def _(d=d):
                for which in range(3):
                    kz(which, z - d).wait_send()

    for d in range(1, ns):
        @pl.when(z - d >= 0)
        def _(d=d):
            kt(0, z - d, m).wait_send()
            kt(1, z - d, m).wait_send()

    def sent_out(t, carry):
        out_copy(t).wait_send()
        return carry

    lax.fori_loop(0, count, sent_out, 0)


def fused_device(
    ns, nf, tokens, h_gain, w_qlat, w_kvlat, w_krope, q_gain, kv_gain, w_uq, w_uk, w_uv,
    w_convb, w_convc, w_convx, conv_taps, w_out_attn, w_out_conv,
):
    half_rows, depth = tokens.shape[1:]
    rows = 2 * half_rows
    slots = ns * nf
    cut = w_qlat.shape[0]
    heads = w_uk.shape[1] // NOPE
    inverse = jnp.tile(THETA ** (-jnp.arange(0, ROPE, 2, dtype=F32) / ROPE), 8)[None]
    vmem = pl.BlockSpec(memory_space=pltpu.VMEM)
    anywhere = pl.BlockSpec(memory_space=pl.ANY)
    V, DMA = pltpu.VMEM, pltpu.SemaphoreType.DMA
    big = (w_convb, w_convc, w_convx, w_uq, w_uk, w_uv, w_out_attn, w_out_conv)
    span = ns * rows
    q_w, kv_w = w_qlat.shape[1] // 2, w_kvlat.shape[1] // 2
    result = pl.pallas_call(
        functools.partial(fused_kernel, ns, nf),
        out_shape=jax.ShapeDtypeStruct((half_rows, depth), BF16),
        in_specs=[vmem] * 9 + [anywhere] * 8,
        out_specs=vmem,
        scratch_shapes=[
            V((half_rows, depth), BF16), V((rows, depth), BF16),
            V((slots, cut, q_w), BF16), V((slots, cut, kv_w), BF16), V((slots, ROPE, cut), BF16),
        ] + [V(w.shape, BF16) for w in big] + [
            V((rows + 8, w_convc.shape[1]), F32),
            V((16, w_convc.shape[1]), BF16), V((16, w_convc.shape[1]), BF16),
            V((rows, w_convc.shape[1]), BF16),
            V((2, rows, kv_w), F32), V((2, rows, q_w), F32),
            V((ns, 2, rows, kv_w), BF16), V((ns, ROPE, rows), BF16),
            V((heads // 2, span, 2 * NOPE), BF16), V((span, 128), BF16),
            V((heads // 2, span, 2 * VH), BF16),
            V((w_uq.shape[0], heads * NOPE), BF16), V((w_uq.shape[0], heads * ROPE), BF16),
            V((rows, 128), F32), V((rows, 128), F32),
            V((heads // 4, rows, 128), BF16), V((heads // 2, rows, 2 * NOPE), BF16),
            V((heads // 2, rows, 2 * VH), BF16),
            V((2, half_rows, depth), BF16), V((half_rows, depth), BF16),
            DMA((8,)), DMA((3, slots, 4)), DMA((3, slots)), DMA((3, slots, 2)),
            DMA((3,)), DMA((3,)), DMA((3, ns)), DMA((3, ns)), DMA((2, ns)), DMA((2, ns)),
            DMA((2,)), DMA((4,)), DMA((4,)),
        ],
        compiler_params=pltpu.CompilerParams(
            collective_id=0, has_side_effects=True, vmem_limit_bytes=60 * 1024 * 1024
        ),
    )(
        tokens[0], h_gain[None], w_qlat, w_kvlat, w_krope.T, q_gain, kv_gain[None],
        conv_taps, inverse, *big,
    )
    return result[None]


def solution(mesh):
    in_specs = (
        P("fs", ("sp", "tp"), None),
        P(),
        P(("sp", "fs"), None),
        P(("sp", "fs"), None),
        P(("sp", "fs"), None),
        P(),
        P(),
        P(None, "tp"),
        P(None, "tp"),
        P(None, "tp"),
        P(None, "tp"),
        P(None, "tp"),
        P(None, "tp"),
        P(None, "tp"),
        P("tp", None),
        P("tp", None),
    )
    out_specs = P("fs", ("sp", "tp"), None)
    fits = mesh.shape["tp"] == 2 and mesh.shape["fs"] == 4
    body = functools.partial(fused_device, mesh.shape["sp"], mesh.shape["fs"]) if fits else per_device
    return jax.shard_map(
        body, mesh=mesh, in_specs=in_specs, out_specs=out_specs, check_vma=False
    )
```
